512 devices in a mesh: grp: 2 (over y), sp: 16 (over z), tp: 16 (over x, core).
Axes of the slice: x: 8, y: 2, z: 16, core: 2. Of those that a mesh axis runs over, the one named last changes fastest.
The devices are a block of a 8x16x16 slice.
Arguments:
- resid: bfloat16 [8192, 2048], P(('grp', 'sp', 'tp')), parts along dimension 0, may hold values from -6 to 6
- gate_b: bfloat16 [8192, 2048], P(('grp', 'sp'), 'tp'), parts along dimension 0, may hold values from -6 to 6
- gate_c: bfloat16 [8192, 2048], P(('grp', 'sp'), 'tp'), parts along dimension 0, may hold values from -6 to 6
- value: bfloat16 [8192, 2048], P(('grp', 'sp'), 'tp'), parts along dimension 0, may hold values from -6 to 6
- taps: bfloat16 [3, 2048], P(None, 'tp'), may hold values from -3.5 to 3.5
- doc_ids: int32 [8192], P(('grp', 'sp')), parts along dimension 0, may hold values from 0 to 3, never falling along the last dimension, each value on 1 to 2048 neighbouring positions
- out_weight: bfloat16 [2048, 2048], P('tp'), may hold values from -0.125 to 0.125
- norm_gains: float32 [3, 2048], replicated, may hold values from 0.1 to 1.9
- routes: int32 [8192, 2], P(('grp', 'sp')), parts along dimension 0, may hold values from 0 to 15, all different within a row; in each aligned block of 16 rows (0 to 15, 16 to 31, ...) at most 3 rows name the same one
- route_weights: float32 [8192, 2], P(('grp', 'sp')), parts along dimension 0, may hold values from 0.2 to 1
- w_gate: bfloat16 [16, 2048, 4096], P('sp', None, 'tp'), may hold values from -0.125 to 0.125
- w_up: bfloat16 [16, 2048, 4096], P('sp', None, 'tp'), may hold values from -0.125 to 0.125
- w_down: bfloat16 [16, 4096, 2048], P('sp', 'tp'), may hold values from -0.09375 to 0.09375
Outputs:
- layer_out: bfloat16 [8192, 2048], P(('grp', 'sp', 'tp')), parts along dimension 0
The draws below stay inside these ranges and needn't reach their ends.
There are 2 independent parts, one for each index of `grp`. The reference program is written for one: setup_inputs(seed, part) draws one part's arguments, and reference() takes and returns one part's arrays. A program takes and returns all parts, laid end to end along the dimension named above; an argument that names none is the same for every part. Nothing has to cross between parts.
Inputs may be any that keep to these rules, and one draw needn't show every extreme that they name: `doc_ids`: never falling along the sequence; each document spans 1 to 2048 positions. `routes`: each row names 2 different experts. In each aligned block of 16 rows no expert is named more than 3 times, and in every draw some block names some expert exactly 3 times.
All inputs are finite; a program needn't handle non-finite values.
Results may differ from the reference program's by a relative error of at most 0.02.
Values may be sent and summed in bfloat16 or wider, within the bound.
A program may use at most 64 MiB of HBM per device.

```python
import math
import jax
import jax.numpy as jnp
import numpy as np
from jax import lax

D = 2048
FF = 4096
TAPS = 3
TOP = 2
TOKENS = 4096
ROWS_BLK = 16
EXPERTS = 16
CAP = 3
DOCS = 4
DOC_MOST = 2048
N_TP = 16


def steps_of(key, dims, cuts, least, high):
    loudness, own = 1.0, jax.random.fold_in(key, 6)
    for position, shards_of in cuts:
        steps = jnp.exp(jax.random.uniform(jax.random.fold_in(own, position), (shards_of,), jnp.float32, least / len(cuts), high / len(cuts)))
        loudness = loudness * jnp.repeat(steps, dims[position] // shards_of).reshape([-1 if axis == position else 1 for axis in range(len(dims))])
    return loudness


def profile(amount, total, most, lean):
    weights = [(1 << 20) // math.isqrt(rank ** lean) + 1 for rank in range(2, amount + 1)]
    rest, counts = total - most - (amount - 1), [1] * (amount - 1)
    while rest > 0:
        movable = [i for i in range(amount - 1) if counts[i] < most]
        whole, budget = sum([weights[i] for i in movable]), rest
        for i in movable:
            more = min(most - counts[i], max(1, budget * weights[i] // whole), rest)
            counts[i] = counts[i] + more
            rest = rest - more
    return np.array([most] + counts)


def uneven(rng, amount, total, reach, slope):
    if amount == 2:
        one = jax.random.randint(rng, (), max(1, total - reach), min(reach, total - 1) + 1)
        return jnp.stack([one, total - one])
    sizes = jnp.asarray(profile(amount, total, reach, slope), jnp.int32)
    twos = (amount - 1) // 2
    source_of, receiver = sizes[1:1 + 2 * twos:2], sizes[2:2 + 2 * twos:2]
    margin = jnp.minimum(source_of - 1, reach - receiver)
    shifted = jax.random.randint(jax.random.fold_in(rng, 1), (twos,), 0, 1 << 20) % (margin + 1)
    sizes = sizes.at[1:1 + 2 * twos:2].set(source_of - shifted).at[2:2 + 2 * twos:2].set(receiver + shifted)
    return sizes[jax.random.permutation(jax.random.fold_in(rng, 2), amount)]


def shared_out(rng, own, number, rows, amount, top, limit, lean):
    sequence = jax.random.permutation(rng, amount)
    packed, common = load_shares(amount, rows * top, limit, lean, True), load_shares(amount, rows * top, limit, lean, False)
    places = jnp.arange(amount)

    def named(lengths, offset_by):
        used = int((lengths > 0).sum())
        fixed = max(1, used // 4)
        shifted = fixed + (places - fixed + offset_by * (used - fixed)) % max(1, amount - fixed)
        return jnp.zeros((amount,), jnp.int32).at[sequence[jnp.where(places < fixed, places, shifted)]].set(jnp.asarray(lengths, jnp.int32))

    lengths = jnp.where(number % 4 == 0, named(packed, number // 4), named(common, number - number // 4 - 1))
    mixed = jax.random.permutation(jax.random.fold_in(own, 3), amount)
    giver, receiver = mixed[0:amount // 2 * 2:2], mixed[1:amount // 2 * 2:2]
    slack = jnp.minimum(lengths[giver] - 1, limit - lengths[receiver]) // 2
    slack = jnp.where((giver == sequence[0]) | (receiver == sequence[0]) | (lengths[receiver] == 0), 0, jnp.maximum(slack, 0))
    shifted = jax.random.randint(jax.random.fold_in(own, 4), (amount // 2,), 0, 1 << 20) % (slack + 1)
    lengths = lengths.at[giver].add(-shifted).at[receiver].add(shifted)
    members = jnp.searchsorted(jnp.cumsum(lengths), jnp.arange(rows * top), side="right").astype(jnp.int32)
    listing = members.reshape(top, rows).T
    listing = listing[jax.random.permutation(jax.random.fold_in(own, 1), rows)]
    offset_by = jax.random.randint(jax.random.fold_in(own, 2), (rows, 1), 0, top)
    return jnp.take_along_axis(listing, (jnp.arange(top)[None, :] + offset_by) % top, axis=1)


def load_shares(amount, total, most, skew, full):
    portions = [(1 << 20) // math.isqrt(standing ** skew) + 1 for standing in range(1, amount + 1)]
    largest = most if full else min(most, max(-(-total // amount), total * portions[0] // sum(portions)))
    least = 1 if total - largest >= amount - 1 else 0
    holding, spare = [largest] + [least] * (amount - 1), total - largest - least * (amount - 1)
    while spare > 0:
        free = [i for i in range(1, amount) if holding[i] < largest] or [i for i in range(1, amount) if holding[i] < most]
        mass, remaining = sum([portions[i] for i in free]), spare
        for i in free:
            extra = min(most - holding[i], max(1, remaining * portions[i] // mass), spare)
            holding[i] = holding[i] + extra
            spare = spare - extra
    return np.array(holding)


def bell_draw(rng, shape, deviation, limit, pieces=(), held_as=jnp.bfloat16):
    values = deviation * jax.random.normal(rng, shape, jnp.float32)
    if pieces:
        values = values * steps_of(rng, shape, pieces, -0.22, 0.18)
    return jnp.clip(values, -limit, limit).astype(held_as)


def setup_inputs(seed: int = 0, part: int = 0) -> dict:
    key_of = jax.random.split(jax.random.key(seed), 14)
    own_keys = jax.random.split(jax.random.fold_in(key_of[13], part), 14)
    resid = bell_draw(own_keys[0], (TOKENS, D), 1.0, 6.0, ((0, 256),))
    gate_b = bell_draw(own_keys[1], (TOKENS, D), 1.0, 6.0, ((0, 16), (1, 16)))
    gate_c = bell_draw(own_keys[2], (TOKENS, D), 1.0, 6.0, ((0, 16), (1, 16)))
    value = bell_draw(own_keys[3], (TOKENS, D), 1.0, 6.0, ((0, 16), (1, 16)))
    taps = bell_draw(key_of[4], (TAPS, D), TAPS ** -0.5, 3.5, ((1, 16),))
    doc_ids = jnp.searchsorted(jnp.cumsum(uneven(own_keys[5], DOCS, TOKENS, DOC_MOST, 1)), jnp.arange(TOKENS), side="right").astype(jnp.int32)
    out_weight = bell_draw(key_of[6], (D, D), D ** -0.5, 0.125, ((0, 16),))
    norm_gains = jnp.clip(1.0 + 0.18 * jax.random.normal(key_of[7], (3, D), jnp.float32), 0.1, 1.9)
    routes_keys = jax.random.split(jax.random.fold_in(own_keys[8], 1), TOKENS // ROWS_BLK)
    routes_turns = jax.random.permutation(jax.random.fold_in(own_keys[8], 3), TOKENS // ROWS_BLK)
    routes = jax.vmap(lambda own, number: shared_out(jax.random.fold_in(own_keys[8], 2), own, number, ROWS_BLK, EXPERTS, TOP, CAP, 1))(routes_keys, routes_turns).reshape((TOKENS, TOP))
    route_weights = jnp.clip(0.2 + 0.8 * jax.random.uniform(own_keys[9], (TOKENS, TOP), jnp.float32) ** steps_of(own_keys[9], (TOKENS, TOP), ((0, 16),), -0.2, 0.2), 0.2, 1.0)
    w_gate = bell_draw(key_of[10], (EXPERTS, D, FF), D ** -0.5, 0.125, ((0, 16), (2, 16)))
    w_up = bell_draw(key_of[11], (EXPERTS, D, FF), D ** -0.5, 0.125, ((0, 16), (2, 16)))
    w_down = bell_draw(key_of[12], (EXPERTS, FF, D), FF ** -0.5, 0.09375, ((0, 16), (1, 16)))
    return {"resid": resid, "gate_b": gate_b, "gate_c": gate_c, "value": value, "taps": taps, "doc_ids": doc_ids, "out_weight": out_weight, "norm_gains": norm_gains, "routes": routes, "route_weights": route_weights, "w_gate": w_gate, "w_up": w_up, "w_down": w_down}


norm_eps = 1e-06

def rms_scale(values, gain_row):
    mean_sq = lax.optimization_barrier(jnp.mean(values * values, axis=-1, keepdims=True))
    return values * lax.rsqrt(mean_sq + norm_eps) * gain_row

def slot_table(block_routes, experts, capacity):
    block_count = block_routes.shape[0]
    block_len = block_routes.shape[1]
    flat_routes = block_routes.reshape(block_count, block_len * TOP)
    onehot = (flat_routes[:, :, None] == jnp.arange(experts, dtype=jnp.int32)[None, None, :]).astype(jnp.int32)
    before = (jnp.cumsum(onehot, axis=1) - onehot).astype(jnp.int32)
    slot_rank = lax.optimization_barrier(jnp.sum(before * onehot, axis=2)).astype(jnp.int32)
    slot_hit = onehot[:, :, :, None] * (slot_rank[:, :, None, None] == jnp.arange(capacity, dtype=jnp.int32)[None, None, None, :]).astype(jnp.int32)
    owner_row = jnp.arange(block_len * TOP, dtype=jnp.int32) // TOP
    slot_tok = lax.optimization_barrier(jnp.sum(slot_hit * owner_row[None, :, None, None], axis=1)).astype(jnp.int32)
    filled = lax.optimization_barrier(jnp.sum(slot_hit, axis=1)).astype(jnp.int32)
    return (slot_rank.reshape(block_count, block_len, TOP), slot_tok, filled)

def grouped_product(left_rows, right_rows, groups):
    group_width = left_rows.shape[1] // groups

    def add_group(running, group_index):
        first = group_index * group_width
        block_cols = lax.dynamic_slice_in_dim(left_rows, first, group_width, 1)
        block_rows = lax.dynamic_slice_in_dim(right_rows, first, group_width, 0)
        group_term = jnp.dot(block_cols, block_rows, preferred_element_type=jnp.float32).astype(jnp.bfloat16)
        group_term = lax.optimization_barrier(group_term)
        return (running + group_term.astype(jnp.float32), None)
    start_sum = jnp.zeros((left_rows.shape[0], right_rows.shape[1]), jnp.float32)
    running, _ = lax.scan(add_group, start_sum, jnp.arange(groups, dtype=jnp.int32))
    return running

def reference(resid, gate_b, gate_c, value, taps, doc_ids, out_weight, norm_gains, routes, route_weights, w_gate, w_up, w_down):
    product = gate_c.astype(jnp.float32) * value.astype(jnp.float32)
    tap_weights = taps.astype(jnp.float32)
    convolved = tap_weights[0] * product
    for distance in range(1, TAPS):
        earlier = jnp.pad(product, ((distance, 0), (0, 0)))[:TOKENS]
        earlier_ids = jnp.pad(doc_ids, (distance, 0), constant_values=-1)[:TOKENS]
        same_doc = earlier_ids == doc_ids
        convolved = convolved + jnp.where(same_doc[:, None], tap_weights[distance] * earlier, 0.0)
    mixed_rows = (gate_b.astype(jnp.float32) * convolved).astype(jnp.bfloat16)
    projected = grouped_product(mixed_rows, out_weight, N_TP)
    gain_rows = norm_gains.astype(jnp.float32)
    stream = resid.astype(jnp.float32) + rms_scale(projected, gain_rows[0])
    normed = rms_scale(stream, gain_rows[1]).astype(jnp.bfloat16)
    blocks = TOKENS // ROWS_BLK
    slot_rank, slot_tok, filled = slot_table(routes.reshape(blocks, ROWS_BLK, TOP), EXPERTS, CAP)
    normed_blocks = normed.reshape(blocks, ROWS_BLK, D)

    def one_expert(expert):
        slot_picks = slot_tok[:, expert]
        slot_live = filled[:, expert]
        picked_rows = jax.vmap(lambda block_rows, picks: block_rows[picks])(normed_blocks, slot_picks)
        picked_rows = jnp.where(slot_live[:, :, None] > 0, picked_rows, jnp.zeros_like(picked_rows))
        picked_rows = picked_rows.reshape(blocks * CAP, D)
        gate_proj = jnp.dot(picked_rows, w_gate[expert], preferred_element_type=jnp.float32)
        up_proj = jnp.dot(picked_rows, w_up[expert], preferred_element_type=jnp.float32)
        hidden = (jax.nn.silu(gate_proj) * up_proj).astype(jnp.bfloat16)
        expert_out = grouped_product(hidden, w_down[expert], N_TP).astype(jnp.bfloat16)
        return expert_out.reshape(blocks, CAP, D)
    expert_out = lax.map(one_expert, jnp.arange(EXPERTS, dtype=jnp.int32))
    block_index = jnp.arange(TOKENS, dtype=jnp.int32) // ROWS_BLK
    picked = expert_out[routes, block_index[:, None], slot_rank.reshape(TOKENS, TOP)]
    shares = route_weights / lax.optimization_barrier(jnp.sum(route_weights, axis=1, keepdims=True))
    combined = lax.optimization_barrier(jnp.sum(shares[:, :, None] * picked.astype(jnp.float32), axis=1))
    return (stream + rms_scale(combined, gain_rows[2])).astype(jnp.bfloat16)
```

```python
import functools

import jax
import jax.numpy as jnp
from jax import lax
from jax.experimental import pallas as pl
from jax.experimental.pallas import tpu as pltpu
from jax.sharding import PartitionSpec as P

TAPS = 3
TOP = 2
LANES = 128
TILE = 16

norm_eps = 1e-06
BF16 = jnp.bfloat16
F32 = jnp.float32
MESH = pl.DeviceIdType.MESH


def rms_scale(values, gain_row):
    mean_sq = jnp.mean(values * values, axis=-1, keepdims=True)
    return values * lax.rsqrt(mean_sq + norm_eps) * gain_row


def layer_kernel(
    n_sp,
    n_tp,
    cap,
    resid,
    gate_b,
    gate_c,
    value,
    taps,
    ids,
    out_w,
    gains,
    routes,
    route_w,
    w_gate,
    w_up,
    w_down,
    out,
    ow,
    wg,
    wu,
    wd,
    ext,
    ext_ids,
    halo_s,
    halo_r,
    mixed,
    sel,
    zs,
    zr,
    bs,
    br,
    fold,
    xbuf,
    hid,
    pair_s,
    pair_r,
    keep,
    ring_s,
    ring_r,
    ring_l,
    stream_ref,
    back,
    w_sem,
    halo_sem,
    z_send,
    z_recv,
    pair_send,
    pair_recv,
    rr_send,
    rr_recv,
    rl_send,
    rl_recv,
    d_send,
    d_recv,
    ar_send,
    ar_recv,
    al_send,
    al_recv,
):
    tok, ch = gate_b.shape
    rows, width = resid.shape
    chips = n_tp // 2
    hops = chips // 2
    half_w = width // 2
    folds = width // LANES
    slots = n_sp * cap
    chunks = slots // TILE
    chunk_rows = n_tp * TILE
    own_rows = chips * TILE
    piece = cap * folds

    tp = lax.axis_index("tp")
    sp = lax.axis_index("sp")
    core = lax.rem(tp, 2)
    chip = lax.div(tp, 2)
    partner = {"tp": chip * 2 + (1 - core)}
    right = {"tp": lax.rem(chip + 1, chips) * 2 + core}
    left = {"tp": lax.rem(chip + chips - 1, chips) * 2 + core}

    def along(d):
        return {"sp": lax.rem(sp + d + n_sp, n_sp)}

    offs = [0] + [
        (p + 1) // 2 if p % 2 else -(p // 2) for p in range(1, n_sp)
    ]

    def pos_of(d):
        return next(p for p in range(n_sp) if (offs[p] - d) % n_sp == 0)

    pending = []

    def send(src, dst, s_sem, r_sem, dev):
        copy = pltpu.make_async_remote_copy(
            src_ref=src,
            dst_ref=dst,
            send_sem=s_sem,
            recv_sem=r_sem,
            device_id=dev,
            device_id_type=MESH,
        )
        copy.start()
        pending.append(copy)
        return copy

    barrier = pltpu.get_barrier_semaphore()
    greeted = [partner, right, left] + [along(d) for d in offs[1:]]
    for dev in greeted:
        pl.semaphore_signal(barrier, inc=1, device_id=dev, device_id_type=MESH)

    loads = [
        pltpu.make_async_copy(out_w, ow, w_sem.at[0]),
        pltpu.make_async_copy(w_gate.at[0], wg, w_sem.at[1]),
        pltpu.make_async_copy(w_up.at[0], wu, w_sem.at[2]),
        pltpu.make_async_copy(w_down.at[0], wd, w_sem.at[3]),
    ]
    for load in loads:
        load.start()

    product = gate_c[...].astype(F32) * value[...].astype(F32)
    ext[pl.ds(8, tok), :] = product
    ext_ids[pl.ds(8, tok), :] = ids[...]
    halo_s[pl.ds(0, 8), :] = product[tok - 8 :]
    halo_s[pl.ds(8, 8), :] = ids[pl.ds(tok - 8, 8), :]

    pl.semaphore_wait(barrier, len(greeted))
    halo = send(halo_s, halo_r, halo_sem.at[0], halo_sem.at[1], along(1))
    halo.wait_recv()
    ext[pl.ds(0, 8), :] = halo_r[pl.ds(0, 8), :]
    ext_ids[pl.ds(0, 8), :] = jnp.where(sp == 0, -1.0, halo_r[pl.ds(8, 8), :])

    here = ext_ids[pl.ds(8, tok), :]
    tap_rows = taps[...].astype(F32)
    conv = tap_rows[0:1, :] * ext[pl.ds(8, tok), :]
    for lag in range(1, TAPS):
        same = ext_ids[pl.ds(8 - lag, tok), :] == here
        conv = conv + jnp.where(
            same, tap_rows[lag : lag + 1, :] * ext[pl.ds(8 - lag, tok), :], 0.0
        )
    mixed[...] = (gate_b[...].astype(F32) * conv).astype(BF16)

    def place(owner, o):
        block = lax.rem(chip + o, chips) * 2 + owner
        return pl.ds(pl.multiple_of(block * rows, rows), rows)

    for o in range(chips):
        sel[0, pl.ds(o * rows, rows), :] = mixed[place(core, o), :]
        sel[1, pl.ds(o * rows, rows), :] = mixed[place(1 - core, o), :]

    ring = {}

    def pair_start(s):
        ring[s, "pair"] = send(
            pair_s.at[s], pair_r.at[s], pair_send.at[s], pair_recv.at[s], partner
        )

    def share(s, o):
        at = pl.ds(o * TILE, TILE)
        return keep[s, at, :] + pair_r[s, at, :].astype(F32)

    def hop_right(s, h, src, dst):
        ring[s, "r", h] = send(
            src, dst, rr_send.at[s, h - 1], rr_recv.at[s, h - 1], right
        )

    def hop_left(s, h, src, dst):
        ring[s, "l", h] = send(
            src, dst, rl_send.at[s, h - 1], rl_recv.at[s, h - 1], left
        )

    lo, hi = pl.ds(0, half_w), pl.ds(half_w, half_w)

    def ring_step(s, h):
        if h == 1:
            ring[s, "pair"].wait_recv()
            ring_s[s, hops] = share(s, hops).astype(BF16)
            hop_right(s, 1, ring_s.at[s, hops, :, lo], ring_r.at[s, 0, :, lo])
            hop_left(s, 1, ring_s.at[s, hops, :, hi], ring_l.at[s, 0, :, hi])
            return
        o = hops + 1 - h
        ring[s, "r", h - 1].wait_recv()
        total = share(s, o)
        if h == 2:
            ring_s[s, o, :, lo] = (
                total[:, :half_w] + ring_r[s, 0, :, lo].astype(F32)
            ).astype(BF16)
            ring_s[s, o, :, hi] = total[:, half_w:].astype(BF16)
        else:
            ring_s[s, o] = (total + ring_r[s, h - 2].astype(F32)).astype(BF16)
        hop_right(s, h, ring_s.at[s, o], ring_r.at[s, h - 1])
        o = chips - o
        ring[s, "l", h - 1].wait_recv()
        total = share(s, o)
        if h == 2:
            ring_s[s, o, :, lo] = total[:, :half_w].astype(BF16)
            ring_s[s, o, :, hi] = (
                total[:, half_w:] + ring_l[s, 0, :, hi].astype(F32)
            ).astype(BF16)
        else:
            ring_s[s, o] = (total + ring_l[s, h - 2].astype(F32)).astype(BF16)
        hop_left(s, h, ring_s.at[s, o], ring_l.at[s, h - 1])

    def ring_end(s):
        ring[s, "r", hops].wait_recv()
        ring[s, "l", hops].wait_recv()
        return (
            share(s, 0)
            + ring_r[s, hops - 1].astype(F32)
            + ring_l[s, hops - 1].astype(F32)
        )

    loads[0].wait()
    step_w = min(512, width)
    for n in range(width // step_w):
        at = pl.ds(n * step_w, step_w)
        pair_s[0, :, at] = jnp.dot(
            sel[1], ow[:, at], preferred_element_type=F32
        ).astype(BF16)
    pair_start(0)
    for n in range(width // step_w):
        at = pl.ds(n * step_w, step_w)
        keep[0, :, at] = jnp.dot(sel[0], ow[:, at], preferred_element_type=F32)
    for h in range(1, hops + 1):
        ring_step(0, h)

    mine = pl.ds(pl.multiple_of(tp * rows, rows), rows)
    my_routes = routes[mine, :]
    my_w = route_w[mine, :]
    lane = lax.broadcasted_iota(jnp.int32, (rows, LANES), 1)
    pos = jnp.floor((lane.astype(F32) + 0.5) * (1.0 / cap)).astype(jnp.int32)
    depth = (lane - pos * cap).astype(F32)
    reach = (pos + 1) >> 1
    away = sp + jnp.where((pos & 1) == 1, reach, -reach)
    away = jnp.where(away < 0, away + n_sp, away)
    away = jnp.where(away >= n_sp, away - n_sp, away)
    expert = jnp.where(lane < slots, away, -1)
    first = (my_routes[:, 0:1] == expert).astype(F32)
    second = (my_routes[:, 1:2] == expert).astype(F32)
    named = first + second
    r_at = lax.broadcasted_iota(jnp.int32, (rows, rows), 0)
    c_at = lax.broadcasted_iota(jnp.int32, (rows, rows), 1)
    earlier = (c_at < r_at).astype(F32).astype(BF16)
    rank = jnp.dot(earlier, named.astype(BF16), preferred_element_type=F32)
    hit = named * (rank == depth).astype(F32)
    total_w = jnp.sum(my_w, axis=1, keepdims=True)
    shares = my_w / total_w
    mix_w = hit * (first * shares[:, 0:1] + second * shares[:, 1:2])
    pick = hit.T.astype(BF16)[:slots, :]

    gain_rows = gains[...]
    projected = ring_end(0)
    stream = resid[...].astype(F32) + rms_scale(projected, gain_rows[0:1, :])
    stream_ref[...] = stream
    normed = rms_scale(stream, gain_rows[1:2, :]).astype(BF16)

    outgoing = jnp.dot(pick, normed, preferred_element_type=F32)
    for b in range(folds):
        fold[pl.ds(b, slots, stride=folds), :] = outgoing[
            :, b * LANES : (b + 1) * LANES
        ]
    folded = fold[...].astype(BF16)
    zs[...] = folded
    zr[pl.ds(0, piece), :] = folded[:piece]

    across = {}

    def z_start(way, src, dst, p):
        q = pos_of(-offs[p])
        across[way, q] = send(
            src.at[pl.ds(p * piece, piece), :],
            dst.at[pl.ds(q * piece, piece), :],
            z_send.at[way, q],
            z_recv.at[way, q],
            along(offs[p]),
        )

    for p in range(1, n_sp):
        z_start(0, zs, zr, p)

    gather = {}
    here_z = [1]

    def block(cc, other, o):
        return pl.ds(cc * chunk_rows + other * own_rows + (o % chips) * TILE, TILE)

    def to_partner(cc, o):
        gather[cc, "d", o % chips] = send(
            xbuf.at[block(cc, 0, o), :],
            xbuf.at[block(cc, 1, o), :],
            d_send.at[cc, o % chips],
            d_recv.at[cc, o % chips],
            partner,
        )

    def hop_out(cc, h):
        if h == 1:
            last = (cc + 1) * TILE * folds
            while here_z[0] < n_sp and here_z[0] * piece < last:
                across[0, here_z[0]].wait_recv()
                here_z[0] += 1
            span = TILE * folds
            fold[pl.ds(0, span), :] = zr[pl.ds(cc * span, span), :].astype(F32)
            for b in range(folds):
                xbuf[block(cc, 0, 0), pl.ds(b * LANES, LANES)] = fold[
                    pl.ds(b, TILE, stride=folds), :
                ].astype(BF16)
        else:
            gather[cc, "r", h - 1].wait_recv()
            gather[cc, "l", h - 1].wait_recv()
        for name, sign, dev, s_sem, r_sem, part in (
            ("r", -1, right, ar_send, ar_recv, lo),
            ("l", 1, left, al_send, al_recv, hi),
        ):
            src = block(cc, 0, sign * (h - 1))
            dst = block(cc, 0, sign * h)
            cols = part if h == hops else slice(None)
            gather[cc, name, h] = send(
                xbuf.at[src, cols],
                xbuf.at[dst, cols],
                s_sem.at[cc, h - 1],
                r_sem.at[cc, h - 1],
                dev,
            )
        to_partner(cc, 1 - h)
        if h > 1:
            to_partner(cc, h - 1)

    def hop_last(cc):
        gather[cc, "r", hops].wait_recv()
        gather[cc, "l", hops].wait_recv()
        to_partner(cc, hops)

    def experts(cc):
        for o in range(chips):
            gather[cc, "d", o].wait_recv()
        s = cc + 1
        x = xbuf[pl.ds(cc * chunk_rows, chunk_rows), :]
        g = jnp.dot(x, wg[...], preferred_element_type=F32)
        u = jnp.dot(x, wu[...], preferred_element_type=F32)
        hid[...] = (g / (1.0 + jnp.exp(-g)) * u).astype(BF16)
        for n in range(width // step_w):
            at = pl.ds(n * step_w, step_w)
            pair_s[s, :, at] = jnp.dot(
                hid[pl.ds(own_rows, own_rows), :],
                wd[:, at],
                preferred_element_type=F32,
            ).astype(BF16)
        pair_start(s)
        for n in range(width // step_w):
            at = pl.ds(n * step_w, step_w)
            keep[s, :, at] = jnp.dot(
                hid[pl.ds(0, own_rows), :], wd[:, at], preferred_element_type=F32
            )

    for load in loads[1:]:
        load.wait()

    for wave in range(hops + chunks):
        for cc in range(chunks):
            h = wave + 1 - cc
            if 1 <= h <= hops:
                hop_out(cc, h)
            elif h == hops + 1:
                hop_last(cc)
        done = wave + 1 - hops - 1
        if 0 <= done < chunks:
            experts(done)

    order = list(range(1, chunks)) + [0]
    finished = set()
    back_sent = set()
    for h in range(1, hops + 1):
        for cc in order:
            ring_step(cc + 1, h)
    for cc in order:
        total = ring_end(cc + 1)
        span = TILE * folds
        for b in range(folds):
            fold[pl.ds(b, TILE, stride=folds), :] = total[
                :, b * LANES : (b + 1) * LANES
            ]
        bs[pl.ds(cc * span, span), :] = fold[pl.ds(0, span), :].astype(BF16)
        finished.add(cc)
        for p in range(1, n_sp):
            needs = {p * piece // span, ((p + 1) * piece - 1) // span}
            if p not in back_sent and needs <= finished:
                back_sent.add(p)
                z_start(1, bs, br, p)
    br[pl.ds(0, piece), :] = bs[pl.ds(0, piece), :]

    for p in range(1, n_sp):
        across[1, p].wait_recv()
    fold[...] = br[...].astype(F32)
    for b in range(folds):
        back[:, pl.ds(b * LANES, LANES)] = fold[
            pl.ds(b, slots, stride=folds), :
        ].astype(BF16)
    mix_w = mix_w[:, :slots]
    mix_hi = mix_w.astype(BF16)
    mix_lo = (mix_w - mix_hi.astype(F32)).astype(BF16)
    picked = back[...]
    combined = jnp.dot(mix_hi, picked, preferred_element_type=F32) + jnp.dot(
        mix_lo, picked, preferred_element_type=F32
    )
    out[...] = (stream_ref[...] + rms_scale(combined, gain_rows[2:3, :])).astype(BF16)

    for copy in pending:
        copy.wait_send()


def per_device(
    resid,
    gate_b,
    gate_c,
    value,
    taps,
    doc_ids,
    out_weight,
    norm_gains,
    routes,
    route_weights,
    w_gate,
    w_up,
    w_down,
):
    n_sp, n_tp = lax.axis_size("sp"), lax.axis_size("tp")
    tok, ch = gate_b.shape
    rows, width = resid.shape
    units = w_gate.shape[2]
    cap = max(2, 3 * TOP * rows // (2 * n_sp))
    chips = n_tp // 2
    hops = chips // 2
    slots = n_sp * cap
    chunks = slots // TILE
    folds = width // LANES
    sets = chunks + 1
    own_rows = chips * TILE
    ids = jnp.broadcast_to(doc_ids.astype(F32)[:, None], (tok, LANES))
    vmem = pl.BlockSpec(memory_space=pltpu.VMEM)
    hbm = pl.BlockSpec(memory_space=pl.ANY)
    dma = pltpu.SemaphoreType.DMA
    return pl.pallas_call(
        functools.partial(layer_kernel, n_sp, n_tp, cap),
        out_shape=jax.ShapeDtypeStruct((rows, width), BF16),
        in_specs=[vmem] * 6 + [hbm] + [vmem] * 3 + [hbm] * 3,
        out_specs=vmem,
        scratch_shapes=[
            pltpu.VMEM(out_weight.shape, BF16),
            pltpu.VMEM(w_gate.shape[1:], BF16),
            pltpu.VMEM(w_up.shape[1:], BF16),
            pltpu.VMEM(w_down.shape[1:], BF16),
            pltpu.VMEM((tok + 8, ch), F32),
            pltpu.VMEM((tok + 8, ch), F32),
            pltpu.VMEM((16, ch), F32),
            pltpu.VMEM((16, ch), F32),
            pltpu.VMEM((tok, ch), BF16),
            pltpu.VMEM((2, own_rows, ch), BF16),
            pltpu.VMEM((slots * folds, LANES), BF16),
            pltpu.VMEM((slots * folds, LANES), BF16),
            pltpu.VMEM((slots * folds, LANES), BF16),
            pltpu.VMEM((slots * folds, LANES), BF16),
            pltpu.VMEM((slots * folds, LANES), F32),
            pltpu.VMEM((chunks * n_tp * TILE, width), BF16),
            pltpu.VMEM((n_tp * TILE, units), BF16),
            pltpu.VMEM((sets, own_rows, width), BF16),
            pltpu.VMEM((sets, own_rows, width), BF16),
            pltpu.VMEM((sets, own_rows, width), F32),
            pltpu.VMEM((sets, chips, TILE, width), BF16),
            pltpu.VMEM((sets, hops, TILE, width), BF16),
            pltpu.VMEM((sets, hops, TILE, width), BF16),
            pltpu.VMEM((rows, width), F32),
            pltpu.VMEM((slots, width), BF16),
            dma((4,)),
            dma((2,)),
            dma((2, n_sp)),
            dma((2, n_sp)),
            dma((sets,)),
            dma((sets,)),
            dma((sets, hops)),
            dma((sets, hops)),
            dma((sets, hops)),
            dma((sets, hops)),
            dma((chunks, chips)),
            dma((chunks, chips)),
            dma((chunks, hops)),
            dma((chunks, hops)),
            dma((chunks, hops)),
            dma((chunks, hops)),
        ],
        compiler_params=pltpu.CompilerParams(
            collective_id=0,
            has_side_effects=True,
            vmem_limit_bytes=56 * 1024 * 1024,
        ),
        name="layer",
    )(
        resid,
        gate_b,
        gate_c,
        value,
        taps,
        ids,
        out_weight,
        norm_gains,
        routes,
        route_weights,
        w_gate,
        w_up,
        w_down,
    )


def solution(mesh):
    return jax.shard_map(
        per_device,
        mesh=mesh,
        in_specs=(
            P(("grp", "sp", "tp"), None),
            P(("grp", "sp"), "tp"),
            P(("grp", "sp"), "tp"),
            P(("grp", "sp"), "tp"),
            P(None, "tp"),
            P(("grp", "sp")),
            P("tp", None),
            P(),
            P(("grp", "sp"), None),
            P(("grp", "sp"), None),
            P("sp", None, "tp"),
            P("sp", None, "tp"),
            P("sp", "tp", None),
        ),
        out_specs=P(("grp", "sp", "tp"), None),
        check_vma=False,
    )
```

```python
import functools

import jax
import jax.numpy as jnp
from jax import lax
from jax.experimental import pallas as pl
from jax.experimental.pallas import tpu as pltpu
from jax.sharding import PartitionSpec as P

TAPS = 3
TOP = 2
LANES = 128
TILE = 16

norm_eps = 1e-06
BF16 = jnp.bfloat16
F32 = jnp.float32
MESH = pl.DeviceIdType.MESH


def rms_scale(values, gain_row):
    mean_sq = jnp.mean(values * values, axis=-1, keepdims=True)
    return values * lax.rsqrt(mean_sq + norm_eps) * gain_row


def layer_kernel(
    n_sp,
    n_tp,
    cap,
    rings,
    resid_h,
    gate_b_h,
    gate_c_h,
    value_h,
    taps_h,
    ids_h,
    out_w_h,
    gains_h,
    routes_h,
    route_w_h,
    w_gate_h,
    w_up_h,
    w_down_h,
    out,
    resid,
    gate_b,
    gate_c,
    value,
    taps,
    ids,
    ow,
    gains,
    routes,
    route_w,
    wg,
    wu,
    wd,
    ext,
    ext_ids,
    halo_s,
    halo_r,
    mixed,
    sel,
    table,
    columns,
    zs,
    zr,
    bs,
    br,
    fold,
    xbuf,
    hid,
    pair_s,
    pair_r,
    keep,
    ring_s,
    ring_r,
    ring_l,
    stream_ref,
    back,
    load_sem,
    halo_sem,
    z_send,
    z_recv,
    back_recv,
    pair_send,
    pair_recv,
    ring_send,
    rr_recv,
    rl_recv,
    gather_send,
    d_recv,
    ar_recv,
    al_recv,
):
    tok, ch = gate_b.shape
    rows, width = resid.shape
    chips = n_tp // 2
    hops = chips // 2
    folds = width // LANES
    slots = n_sp * cap
    chunks = slots // TILE
    chunk_rows = n_tp * TILE
    own_rows = chips * TILE
    piece = cap * folds
    span = TILE * folds

    tp = lax.axis_index("tp")
    sp = lax.axis_index("sp")
    core = lax.rem(tp, 2)
    chip = lax.div(tp, 2)
    partner = {"tp": chip * 2 + (1 - core)}
    right = {"tp": lax.rem(chip + 1, chips) * 2 + core}
    left = {"tp": lax.rem(chip + chips - 1, chips) * 2 + core}

    def along(d):
        return {"sp": lax.rem(sp + d + n_sp, n_sp)}

    offs = [0] + [
        (p + 1) // 2 if p % 2 else -(p // 2) for p in range(1, n_sp)
    ]

    def pos_of(d):
        return next(p for p in range(n_sp) if (offs[p] - d) % n_sp == 0)

    def remote(src, dst, s_sem, r_sem, dev):
        return pltpu.make_async_remote_copy(
            src_ref=src,
            dst_ref=dst,
            send_sem=s_sem,
            recv_sem=r_sem,
            device_id=dev,
            device_id_type=MESH,
        )

    def send(src, dst, s_sem, r_sem, dev):
        copy = remote(src, dst, s_sem, r_sem, dev)
        copy.start()
        return copy

    def settle(ref, sem):
        pltpu.make_async_copy(ref, ref, sem).wait()

    barrier = pltpu.get_barrier_semaphore()
    greeted = [partner, right, left] + [along(d) for d in offs[1:]]
    for dev in greeted:
        pl.semaphore_signal(barrier, inc=1, device_id=dev, device_id_type=MESH)

    loads = {}
    for i, (name, src, dst) in enumerate(
        (
            ("ids", ids_h, ids),
            ("gate_c", gate_c_h, gate_c),
            ("value", value_h, value),
            ("gate_b", gate_b_h, gate_b),
            ("taps", taps_h, taps),
            ("ow", out_w_h, ow),
            ("routes", routes_h, routes),
            ("route_w", route_w_h, route_w),
            ("gains", gains_h, gains),
            ("resid", resid_h, resid),
            ("wg", w_gate_h.at[0], wg),
            ("wu", w_up_h.at[0], wu),
            ("wd", w_down_h.at[0], wd),
        )
    ):
        loads[name] = pltpu.make_async_copy(src, dst, load_sem.at[i])
        loads[name].start()

    parts = tok // LANES
    loads["ids"].wait()
    for k in range(parts):
        line = ids[k : k + 1, :].astype(F32)
        ext_ids[pl.ds(8 + k * LANES, LANES), :] = jnp.broadcast_to(
            line, (LANES, LANES)
        ).T
    loads["gate_c"].wait()
    loads["value"].wait()
    product = gate_c[...].astype(F32) * value[...].astype(F32)
    ext[pl.ds(8, tok), :] = product
    halo_s[pl.ds(0, 8), :] = product[tok - 8 :]
    halo_s[pl.ds(8, 8), :] = ext_ids[pl.ds(tok, 8), :]

    with jax.named_scope("barrier"):
        pl.semaphore_wait(barrier, len(greeted))
    halo = remote(halo_s, halo_r, halo_sem.at[0], halo_sem.at[1], along(1))

    @pl.when(sp < n_sp - 1)
    def _():
        halo.start()

    ext[pl.ds(0, 8), :] = jnp.zeros((8, ch), F32)
    ext_ids[pl.ds(0, 8), :] = jnp.full((8, LANES), -1.0, F32)
    loads["gate_b"].wait()
    loads["taps"].wait()

    @pl.when(sp > 0)
    def _():
        halo.wait_recv()
        ext[pl.ds(0, 8), :] = halo_r[pl.ds(0, 8), :]
        ext_ids[pl.ds(0, 8), :] = halo_r[pl.ds(8, 8), :]

    here = ext_ids[pl.ds(8, tok), :]
    tap_rows = taps[...].astype(F32)
    conv = tap_rows[0:1, :] * ext[pl.ds(8, tok), :]
    for lag in range(1, TAPS):
        same = ext_ids[pl.ds(8 - lag, tok), :] == here
        conv = conv + jnp.where(
            same, tap_rows[lag : lag + 1, :] * ext[pl.ds(8 - lag, tok), :], 0.0
        )
    mixed[...] = (gate_b[...].astype(F32) * conv).astype(BF16)

    def place(owner, o):
        block = lax.rem(chip + o, chips) * 2 + owner
        return pl.ds(pl.multiple_of(block * rows, rows), rows)

    for o in range(chips):
        sel[0, pl.ds(o * rows, rows), :] = mixed[place(core, o), :]
        sel[1, pl.ds(o * rows, rows), :] = mixed[place(1 - core, o), :]

    ring = {}

    def pair_start(k):
        s, at, cols = rings[k]
        at = pl.ds(at, cols)
        ring[k, "pair"] = send(
            pair_s.at[s, :, at],
            pair_r.at[s, :, at],
            pair_send.at[0],
            pair_recv.at[k],
            partner,
        )

    def ring_step(k, h):
        with jax.named_scope(f"rs{k}_{h}"):
            ring_hop(k, h)

    def ring_hop(k, h):
        s, at, cols = rings[k]
        all_c = pl.ds(at, cols)
        lo, hi = pl.ds(at, cols // 2), pl.ds(at + cols // 2, cols // 2)

        def share(o, c):
            r = pl.ds(o * TILE, TILE)
            return keep[s, r, c] + pair_r[s, r, c].astype(F32)

        if h == 1:
            ring[k, "pair"].wait_recv()
            ring_s[s, hops, :, all_c] = share(hops, all_c).astype(BF16)
        for name, buf, sem, dev, early, late in (
            ("r", ring_r, rr_recv, right, lo, hi),
            ("l", ring_l, rl_recv, left, hi, lo),
        ):
            o = hops + 1 - h
            if name == "l":
                o = (chips - o) % chips
            if h > 1:
                ring[k, name, h - 1].wait_recv()
            if h == 2:
                ring_s[s, o, :, early] = (
                    share(o, early) + buf[s, 0, :, early].astype(F32)
                ).astype(BF16)
                ring_s[s, o, :, late] = share(o, late).astype(BF16)
            elif h > 2:
                ring_s[s, o, :, all_c] = (
                    share(o, all_c) + buf[s, h - 2, :, all_c].astype(F32)
                ).astype(BF16)
            c = early if h == 1 else all_c
            ring[k, name, h] = send(
                ring_s.at[s, o, :, c],
                buf.at[s, h - 1, :, c],
                ring_send.at[0],
                sem.at[k, h - 1],
                dev,
            )

    def ring_end(k):
        with jax.named_scope(f"re{k}"):
            s, at, cols = rings[k]
            c = pl.ds(at, cols)
            ring[k, "r", hops].wait_recv()
            ring[k, "l", hops].wait_recv()
            return (
                keep[s, pl.ds(0, TILE), c]
                + pair_r[s, pl.ds(0, TILE), c].astype(F32)
                + ring_r[s, hops - 1, :, c].astype(F32)
                + ring_l[s, hops - 1, :, c].astype(F32)
            )

    first_rings = [k for k in range(len(rings)) if rings[k][0] == 0]
    loads["ow"].wait()
    step_w = min(512, width)
    for k in first_rings:
        _, at, cols = rings[k]
        for n in range(cols // step_w):
            c = pl.ds(at + n * step_w, step_w)
            pair_s[0, :, c] = jnp.dot(
                sel[1], ow[:, c], preferred_element_type=F32
            ).astype(BF16)
        pair_start(k)
    for n in range(width // step_w):
        c = pl.ds(n * step_w, step_w)
        keep[0, :, c] = jnp.dot(sel[0], ow[:, c], preferred_element_type=F32)
    for h in range(1, hops + 1):
        for k in first_rings:
            ring_step(k, h)

    loads["routes"].wait()
    loads["route_w"].wait()
    for k in range(TOP):
        for part in range(parts):
            c = pl.ds(part * LANES, LANES)
            table[pl.ds(k * parts + part, 1), :] = routes[pl.ds(k, 1), c].astype(F32)
            table[pl.ds((TOP + k) * parts + part, 1), :] = route_w[pl.ds(k, 1), c]
    columns[:, pl.ds(0, 2 * TOP * parts)] = table[...].T
    base = tp * rows
    my_part = lax.div(base, LANES)
    mine = columns[pl.ds(pl.multiple_of(base - my_part * LANES, rows), rows), :]

    def column(n):
        found = mine[:, n * parts : n * parts + 1]
        for part in range(1, parts):
            found = jnp.where(
                my_part == part, mine[:, n * parts + part : n * parts + part + 1], found
            )
        return found

    lane = lax.broadcasted_iota(jnp.int32, (rows, LANES), 1)
    pos = jnp.floor((lane.astype(F32) + 0.5) * (1.0 / cap)).astype(jnp.int32)
    depth = (lane - pos * cap).astype(F32)
    reach = (pos + 1) >> 1
    away = sp + jnp.where((pos & 1) == 1, reach, -reach)
    away = jnp.where(away < 0, away + n_sp, away)
    away = jnp.where(away >= n_sp, away - n_sp, away)
    expert = jnp.where(lane < slots, away, -1).astype(F32)
    first = (column(0) == expert).astype(F32)
    second = (column(1) == expert).astype(F32)
    named = first + second
    r_at = lax.broadcasted_iota(jnp.int32, (rows, rows), 0)
    c_at = lax.broadcasted_iota(jnp.int32, (rows, rows), 1)
    earlier = (c_at < r_at).astype(F32).astype(BF16)
    rank = jnp.dot(earlier, named.astype(BF16), preferred_element_type=F32)
    hit = named * (rank == depth).astype(F32)
    w_first, w_second = column(TOP), column(TOP + 1)
    w_sum = w_first + w_second
    mix_w = hit * (first * (w_first / w_sum) + second * (w_second / w_sum))
    pick = hit.T.astype(BF16)[:slots, :]

    loads["gains"].wait()
    loads["resid"].wait()
    gain_rows = gains[...]
    projected = jnp.concatenate([ring_end(k) for k in first_rings], axis=1)
    stream = resid[...].astype(F32) + rms_scale(projected, gain_rows[0:1, :])
    stream_ref[...] = stream
    normed = rms_scale(stream, gain_rows[1:2, :]).astype(BF16)

    outgoing = jnp.dot(pick, normed, preferred_element_type=F32)
    for b in range(folds):
        fold[pl.ds(b, slots, stride=folds), :] = outgoing[
            :, b * LANES : (b + 1) * LANES
        ]
    folded = fold[...].astype(BF16)
    zs[...] = folded
    zr[pl.ds(0, piece), :] = folded[:piece]

    group_of = [(p * piece) // span for p in range(n_sp)]

    def z_start(way, src, dst, p):
        q = pos_of(-offs[p])
        sem = z_recv.at[group_of[q]] if way == 0 else back_recv.at[0]
        send(
            src.at[pl.ds(p * piece, piece), :],
            dst.at[pl.ds(q * piece, piece), :],
            z_send.at[way],
            sem,
            along(offs[p]),
        )

    for p in reversed(range(1, n_sp)):
        z_start(0, zs, zr, p)

    gather = {}
    came = set()

    def block(cc, other, o):
        return pl.ds(cc * chunk_rows + other * own_rows + (o % chips) * TILE, TILE)

    def to_partner(cc, o):
        send(
            xbuf.at[block(cc, 0, o), :],
            xbuf.at[block(cc, 1, o), :],
            gather_send.at[0],
            d_recv.at[cc],
            partner,
        )

    def hop_out(cc, h):
        with jax.named_scope(f"ag{cc}_{h}"):
            gather_hop(cc, h)

    def gather_hop(cc, h):
        if h == 1:
            for g in range(cc + 1):
                here_p = [p for p in range(1, n_sp) if group_of[p] == g]
                if g not in came and here_p[0] * piece < (cc + 1) * span and (
                    (here_p[-1] + 1) * piece > cc * span
                ):
                    came.add(g)
                    settle(
                        zr.at[pl.ds(here_p[0] * piece, len(here_p) * piece), :],
                        z_recv.at[g],
                    )
            fold[pl.ds(0, span), :] = zr[pl.ds(cc * span, span), :].astype(F32)
            for b in range(folds):
                xbuf[block(cc, 0, 0), pl.ds(b * LANES, LANES)] = fold[
                    pl.ds(b, TILE, stride=folds), :
                ].astype(BF16)
        else:
            gather[cc, "r", h - 1].wait_recv()
            gather[cc, "l", h - 1].wait_recv()
        for name, sign, dev, sem, at in (
            ("r", -1, right, ar_recv, 0),
            ("l", 1, left, al_recv, width // 2),
        ):
            c = pl.ds(at, width // 2) if h == hops else slice(None)
            gather[cc, name, h] = send(
                xbuf.at[block(cc, 0, sign * (h - 1)), c],
                xbuf.at[block(cc, 0, sign * h), c],
                gather_send.at[0],
                sem.at[cc, h - 1],
                dev,
            )
        to_partner(cc, 1 - h)
        if h > 1:
            to_partner(cc, h - 1)

    def hop_last(cc):
        with jax.named_scope(f"agl{cc}"):
            gather[cc, "r", hops].wait_recv()
            gather[cc, "l", hops].wait_recv()
            to_partner(cc, hops)

    def experts(cc):
        s = cc + 1
        k = next(k for k in range(len(rings)) if rings[k][0] == s)
        with jax.named_scope(f"exw{cc}"):
            settle(
                xbuf.at[pl.ds(cc * chunk_rows + own_rows, own_rows), :], d_recv.at[cc]
            )
        with jax.named_scope(f"exc{cc}"):
            x = xbuf[pl.ds(cc * chunk_rows, chunk_rows), :]
            g = jnp.dot(x, wg[...], preferred_element_type=F32)
            u = jnp.dot(x, wu[...], preferred_element_type=F32)
            hid[...] = (g / (1.0 + jnp.exp(-g)) * u).astype(BF16)
            for n in range(width // step_w):
                c = pl.ds(n * step_w, step_w)
                pair_s[s, :, c] = jnp.dot(
                    hid[pl.ds(own_rows, own_rows), :],
                    wd[:, c],
                    preferred_element_type=F32,
                ).astype(BF16)
            pair_start(k)
            for n in range(width // step_w):
                c = pl.ds(n * step_w, step_w)
                keep[s, :, c] = jnp.dot(
                    hid[pl.ds(0, own_rows), :], wd[:, c], preferred_element_type=F32
                )
        return k

    order = list(reversed(range(chunks)))
    for h in range(1, hops + 1):
        for cc in order:
            hop_out(cc, h)
    for name in ("wg", "wu", "wd"):
        loads[name].wait()
    ring_of = {}
    for i, cc in enumerate(order):
        if i == 0:
            hop_last(cc)
        if i + 1 < chunks:
            hop_last(order[i + 1])
        ring_of[cc] = experts(cc)
        if i > 0:
            ring_step(ring_of[order[i - 1]], 1)
    ring_step(ring_of[order[-1]], 1)
    for h in range(2, hops + 1):
        for cc in order:
            ring_step(ring_of[cc], h)

    finished = set()
    back_sent = set()
    for cc in order:
        total = ring_end(ring_of[cc])
        for b in range(folds):
            fold[pl.ds(b, TILE, stride=folds), :] = total[
                :, b * LANES : (b + 1) * LANES
            ]
        bs[pl.ds(cc * span, span), :] = fold[pl.ds(0, span), :].astype(BF16)
        finished.add(cc)
        for p in reversed(range(1, n_sp)):
            needs = {p * piece // span, ((p + 1) * piece - 1) // span}
            if p not in back_sent and needs <= finished:
                back_sent.add(p)
                z_start(1, bs, br, p)
    br[pl.ds(0, piece), :] = bs[pl.ds(0, piece), :]

    far = (n_sp - 1) * piece
    ring_rows = (2 * hops - 1) * TILE
    with jax.named_scope("sendwait"):
        settle(pair_s, pair_send.at[0])
        settle(pair_s.at[:, pl.ds(0, ring_rows), :], ring_send.at[0])
        settle(
            xbuf.at[pl.ds(0, chunks * (ring_rows + own_rows)), :], gather_send.at[0]
        )
        settle(zs.at[pl.ds(piece, far), :], z_send.at[0])

        @pl.when(sp < n_sp - 1)
        def _():
            halo.wait_send()

    with jax.named_scope("backwait"):
        settle(br.at[pl.ds(piece, far), :], back_recv.at[0])
    fold[...] = br[...].astype(F32)
    for b in range(folds):
        back[:, pl.ds(b * LANES, LANES)] = fold[
            pl.ds(b, slots, stride=folds), :
        ].astype(BF16)
    mix_w = mix_w[:, :slots]
    mix_hi = mix_w.astype(BF16)
    mix_lo = (mix_w - mix_hi.astype(F32)).astype(BF16)
    picked = back[...]
    combined = jnp.dot(mix_hi, picked, preferred_element_type=F32) + jnp.dot(
        mix_lo, picked, preferred_element_type=F32
    )
    out[...] = stream_ref[...] + rms_scale(combined, gain_rows[2:3, :])
    settle(bs.at[pl.ds(piece, far), :], z_send.at[1])


def per_device(
    resid,
    gate_b,
    gate_c,
    value,
    taps,
    doc_ids,
    out_weight,
    norm_gains,
    routes,
    route_weights,
    w_gate,
    w_up,
    w_down,
):
    n_sp, n_tp = lax.axis_size("sp"), lax.axis_size("tp")
    tok, ch = gate_b.shape
    rows, width = resid.shape
    units = w_gate.shape[2]
    cap = max(2, 3 * TOP * rows // (2 * n_sp))
    chips = n_tp // 2
    hops = chips // 2
    slots = n_sp * cap
    chunks = slots // TILE
    folds = width // LANES
    sets = chunks + 1
    own_rows = chips * TILE
    parts = tok // LANES
    rings = [(0, 0, width // 2), (0, width // 2, width // 2)]
    rings += [(s, 0, width) for s in range(1, sets)]
    n_rings = len(rings)
    operands = (
        resid,
        gate_b,
        gate_c,
        value,
        taps,
        doc_ids.reshape(parts, LANES),
        out_weight,
        norm_gains,
        routes.T,
        route_weights.T,
        w_gate,
        w_up,
        w_down,
    )
    hbm = pl.BlockSpec(memory_space=pl.ANY)
    vmem = pltpu.VMEM
    dma = pltpu.SemaphoreType.DMA
    result = pl.pallas_call(
        functools.partial(layer_kernel, n_sp, n_tp, cap, rings),
        out_shape=jax.ShapeDtypeStruct((rows, width), F32),
        in_specs=[hbm] * len(operands),
        out_specs=pl.BlockSpec(memory_space=vmem),
        scratch_shapes=[
            *[vmem(a.shape, a.dtype) for a in operands[:10]],
            *[vmem(a.shape[1:], a.dtype) for a in operands[10:]],
            vmem((tok + 8, ch), F32),
            vmem((tok + 8, LANES), F32),
            vmem((16, ch), F32),
            vmem((16, ch), F32),
            vmem((tok, ch), BF16),
            vmem((2, own_rows, ch), BF16),
            vmem((2 * TOP * parts, LANES), F32),
            vmem((LANES, LANES), F32),
            vmem((slots * folds, LANES), BF16),
            vmem((slots * folds, LANES), BF16),
            vmem((slots * folds, LANES), BF16),
            vmem((slots * folds, LANES), BF16),
            vmem((slots * folds, LANES), F32),
            vmem((chunks * n_tp * TILE, width), BF16),
            vmem((n_tp * TILE, units), BF16),
            vmem((sets, own_rows, width), BF16),
            vmem((sets, own_rows, width), BF16),
            vmem((sets, own_rows, width), F32),
            vmem((sets, chips, TILE, width), BF16),
            vmem((sets, hops, TILE, width), BF16),
            vmem((sets, hops, TILE, width), BF16),
            vmem((rows, width), F32),
            vmem((slots, width), BF16),
            dma((len(operands),)),
            dma((2,)),
            dma((2,)),
            dma((chunks,)),
            dma((1,)),
            dma((1,)),
            dma((n_rings,)),
            dma((1,)),
            dma((n_rings, hops)),
            dma((n_rings, hops)),
            dma((1,)),
            dma((chunks,)),
            dma((chunks, hops)),
            dma((chunks, hops)),
        ],
        compiler_params=pltpu.CompilerParams(
            collective_id=0,
            has_side_effects=True,
            vmem_limit_bytes=56 * 1024 * 1024,
        ),
        name="layer",
    )(*operands)
    return result.astype(BF16)


def solution(mesh):
    return jax.shard_map(
        per_device,
        mesh=mesh,
        in_specs=(
            P(("grp", "sp", "tp"), None),
            P(("grp", "sp"), "tp"),
            P(("grp", "sp"), "tp"),
            P(("grp", "sp"), "tp"),
            P(None, "tp"),
            P(("grp", "sp")),
            P("tp", None),
            P(),
            P(("grp", "sp"), None),
            P(("grp", "sp"), None),
            P("sp", None, "tp"),
            P("sp", None, "tp"),
            P("sp", "tp", None),
        ),
        out_specs=P(("grp", "sp", "tp"), None),
        check_vma=False,
    )
```

```python
import functools

import jax
import jax.numpy as jnp
from jax import lax
from jax.experimental import pallas as pl
from jax.experimental.pallas import tpu as pltpu
from jax.sharding import PartitionSpec as P

TAPS = 3
TOP = 2
LANES = 128
TILE = 16

norm_eps = 1e-06

ORDER = (
    (0, 0, 0, 1), (0, 0, 1, 1), (0, 1, 0, 1), (0, 1, 1, 1), (0, 0, 0, 2),
    (0, 0, 1, 2), (0, 1, 0, 2), (0, 1, 1, 2), (0, 0, 0, 3), (0, 0, 1, 3),
    (0, 1, 0, 3), (0, 2, 0, 1), (0, 2, 1, 1), (0, 0, 0, 4), (0, 1, 1, 3),
    (0, 0, 1, 4), (0, 1, 0, 4), (0, 2, 0, 2), (0, 2, 1, 2), (4, 0, 0),
    (4, 0, 1), (4, 1, 0), (0, 2, 0, 3), (0, 2, 1, 3), (0, 1, 1, 4),
    (1, 0), (0, 2, 0, 4), (0, 2, 1, 4), (4, 1, 1), (2, 0, 0, 1),
    (2, 0, 1, 1), (4, 2, 0), (4, 2, 1), (2, 0, 0, 2), (2, 0, 1, 2),
    (1, 2), (1, 1), (2, 2, 0, 1), (2, 2, 1, 1), (2, 1, 0, 1),
    (2, 1, 1, 1), (2, 0, 0, 3), (2, 0, 1, 3), (2, 2, 0, 2), (2, 2, 1, 2),
    (2, 1, 0, 2), (2, 1, 1, 2), (2, 0, 0, 4), (2, 2, 0, 3), (2, 2, 1, 3),
    (2, 1, 0, 3), (2, 1, 1, 3), (3, 0, 0), (2, 2, 0, 4), (2, 2, 1, 4),
    (2, 1, 0, 4), (2, 1, 1, 4), (2, 0, 1, 4), (3, 2, 0), (3, 2, 1),
    (3, 1, 0), (3, 1, 1), (3, 0, 1),
)
BF16 = jnp.bfloat16
F32 = jnp.float32
MESH = pl.DeviceIdType.MESH


def rms_scale(values, gain_row):
    mean_sq = jnp.mean(values * values, axis=-1, keepdims=True)
    return values * lax.rsqrt(mean_sq + norm_eps) * gain_row


def layer_kernel(
    n_sp,
    n_tp,
    cap,
    rings,
    resid_h,
    gate_b_h,
    gate_c_h,
    value_h,
    taps_h,
    ids_h,
    out_w_h,
    gains_h,
    routes_h,
    route_w_h,
    w_gate_h,
    w_up_h,
    w_down_h,
    out,
    resid,
    gate_b,
    gate_c,
    value,
    taps,
    ids,
    ow,
    gains,
    routes,
    route_w,
    wg,
    wu,
    wd,
    ext,
    ext_ids,
    halo_s,
    halo_r,
    mixed,
    sel,
    table,
    columns,
    zs,
    zr,
    bs,
    br,
    fold,
    xbuf,
    hid,
    pair_s,
    pair_r,
    keep,
    ring_s,
    ring_r,
    ring_l,
    stream_ref,
    back,
    load_sem,
    halo_sem,
    below_sem,
    above_sem,
    z_send,
    z_recv,
    back_recv,
    pair_send,
    pair_recv,
    ring_send,
    rr_recv,
    rl_recv,
    gather_send,
    d_recv,
    ar_recv,
    al_recv,
):
    tok, ch = gate_b.shape
    rows, width = resid.shape
    chips = n_tp // 2
    hops = chips // 2
    folds = width // LANES
    slots = n_sp * cap
    chunks = slots // TILE
    chunk_rows = n_tp * TILE
    own_rows = chips * TILE
    piece = cap * folds
    span = TILE * folds

    tp = lax.axis_index("tp")
    sp = lax.axis_index("sp")
    core = lax.rem(tp, 2)
    chip = lax.div(tp, 2)
    partner = {"tp": chip * 2 + (1 - core)}
    right = {"tp": lax.rem(chip + 1, chips) * 2 + core}
    left = {"tp": lax.rem(chip + chips - 1, chips) * 2 + core}

    def along(d):
        return {"sp": lax.rem(sp + d + n_sp, n_sp)}

    def remote(src, dst, s_sem, r_sem, dev):
        return pltpu.make_async_remote_copy(
            src_ref=src,
            dst_ref=dst,
            send_sem=s_sem,
            recv_sem=r_sem,
            device_id=dev,
            device_id_type=MESH,
        )

    def send(src, dst, s_sem, r_sem, dev):
        copy = remote(src, dst, s_sem, r_sem, dev)
        copy.start()
        return copy

    def settle(ref, sem):
        pltpu.make_async_copy(ref, ref, sem).wait()

    barrier = pltpu.get_barrier_semaphore()
    greeted = [partner, right, left]
    for dev in greeted:
        pl.semaphore_signal(barrier, inc=1, device_id=dev, device_id_type=MESH)
    has_below, has_above = sp > 0, sp < n_sp - 1

    @pl.when(has_below)
    def _():
        pl.semaphore_signal(barrier, inc=1, device_id=along(-1), device_id_type=MESH)

    @pl.when(has_above)
    def _():
        pl.semaphore_signal(barrier, inc=1, device_id=along(1), device_id_type=MESH)

    loads = {}
    for i, (name, src, dst) in enumerate(
        (
            ("ids", ids_h, ids),
            ("gate_c", gate_c_h, gate_c),
            ("value", value_h, value),
            ("gate_b", gate_b_h, gate_b),
            ("taps", taps_h, taps),
            ("ow", out_w_h, ow),
            ("routes", routes_h, routes),
            ("route_w", route_w_h, route_w),
            ("gains", gains_h, gains),
            ("resid", resid_h, resid),
            ("wg", w_gate_h.at[0], wg),
            ("wu", w_up_h.at[0], wu),
            ("wd", w_down_h.at[0], wd),
        )
    ):
        loads[name] = pltpu.make_async_copy(src, dst, load_sem.at[i])
        loads[name].start()

    parts = tok // LANES
    loads["ids"].wait()
    for k in range(parts):
        line = ids[k : k + 1, :].astype(F32)
        ext_ids[pl.ds(8 + k * LANES, LANES), :] = jnp.broadcast_to(
            line, (LANES, LANES)
        ).T
    loads["gate_c"].wait()
    loads["value"].wait()
    product = gate_c[...].astype(F32) * value[...].astype(F32)
    ext[pl.ds(8, tok), :] = product
    halo_s[pl.ds(0, 8), :] = product[tok - 8 :]
    halo_s[pl.ds(8, 8), :] = ext_ids[pl.ds(tok, 8), :]

    with jax.named_scope("barrier"):
        pl.semaphore_wait(
            barrier,
            len(greeted) + jnp.where(has_below, 1, 0) + jnp.where(has_above, 1, 0),
        )
    halo = remote(halo_s, halo_r, halo_sem.at[0], halo_sem.at[1], along(1))

    @pl.when(has_above)
    def _():
        halo.start()

    ext[pl.ds(0, 8), :] = jnp.zeros((8, ch), F32)
    ext_ids[pl.ds(0, 8), :] = jnp.full((8, LANES), -1.0, F32)
    loads["gate_b"].wait()
    loads["taps"].wait()

    @pl.when(has_below)
    def _():
        halo.wait_recv()
        ext[pl.ds(0, 8), :] = halo_r[pl.ds(0, 8), :]
        ext_ids[pl.ds(0, 8), :] = halo_r[pl.ds(8, 8), :]

    @pl.when(has_below)
    def _():
        pl.semaphore_wait(below_sem, 1)

    @pl.when(has_above)
    def _():
        pl.semaphore_signal(
            below_sem, inc=1, device_id=along(1), device_id_type=MESH
        )

    for d in range(1, n_sp):

        @pl.when(sp >= d)
        def _():
            pl.semaphore_signal(
                above_sem, inc=1, device_id=along(-d), device_id_type=MESH
            )

    here = ext_ids[pl.ds(8, tok), :]
    tap_rows = taps[...].astype(F32)
    conv = tap_rows[0:1, :] * ext[pl.ds(8, tok), :]
    for lag in range(1, TAPS):
        same = ext_ids[pl.ds(8 - lag, tok), :] == here
        conv = conv + jnp.where(
            same, tap_rows[lag : lag + 1, :] * ext[pl.ds(8 - lag, tok), :], 0.0
        )
    mixed[...] = (gate_b[...].astype(F32) * conv).astype(BF16)

    def place(owner, o):
        block = lax.rem(chip + o, chips) * 2 + owner
        return pl.ds(pl.multiple_of(block * rows, rows), rows)

    for o in range(chips):
        sel[0, pl.ds(o * rows, rows), :] = mixed[place(core, o), :]
        sel[1, pl.ds(o * rows, rows), :] = mixed[place(1 - core, o), :]

    ring = {}

    def pair_start(k):
        s, at, cols = rings[k]
        at = pl.ds(at, cols)
        ring[k, "pair"] = send(
            pair_s.at[s, :, at],
            pair_r.at[s, :, at],
            pair_send.at[0],
            pair_recv.at[k],
            partner,
        )

    def ring_step(k, h):
        with jax.named_scope(f"rs{k}_{h}"):
            ring_hop(k, h)

    def ring_hop(k, h):
        s, at, cols = rings[k]
        all_c = pl.ds(at, cols)
        lo, hi = pl.ds(at, cols // 2), pl.ds(at + cols // 2, cols // 2)

        def share(o, c):
            r = pl.ds(o * TILE, TILE)
            return keep[s, r, c] + pair_r[s, r, c].astype(F32)

        if h == 1:
            ring[k, "pair"].wait_recv()
            ring_s[s, hops, :, all_c] = share(hops, all_c).astype(BF16)
        for name, buf, sem, dev, early, late in (
            ("r", ring_r, rr_recv, right, lo, hi),
            ("l", ring_l, rl_recv, left, hi, lo),
        ):
            o = hops + 1 - h
            if name == "l":
                o = (chips - o) % chips
            if h > 1:
                ring[k, name, h - 1].wait_recv()
            if h == 2:
                ring_s[s, o, :, early] = (
                    share(o, early) + buf[s, 0, :, early].astype(F32)
                ).astype(BF16)
                ring_s[s, o, :, late] = share(o, late).astype(BF16)
            elif h > 2:
                ring_s[s, o, :, all_c] = (
                    share(o, all_c) + buf[s, h - 2, :, all_c].astype(F32)
                ).astype(BF16)
            c = early if h == 1 else all_c
            ring[k, name, h] = send(
                ring_s.at[s, o, :, c],
                buf.at[s, h - 1, :, c],
                ring_send.at[0],
                sem.at[k, h - 1],
                dev,
            )

    def ring_end(k):
        with jax.named_scope(f"re{k}"):
            s, at, cols = rings[k]
            c = pl.ds(at, cols)
            ring[k, "r", hops].wait_recv()
            ring[k, "l", hops].wait_recv()
            return (
                keep[s, pl.ds(0, TILE), c]
                + pair_r[s, pl.ds(0, TILE), c].astype(F32)
                + ring_r[s, hops - 1, :, c].astype(F32)
                + ring_l[s, hops - 1, :, c].astype(F32)
            )

    set_rings = {}
    for k, (s, _, _) in enumerate(rings):
        set_rings.setdefault(s, []).append(k)
    first_rings = set_rings[0]
    loads["ow"].wait()
    step_w = min(512, width)
    for k in first_rings:
        _, at, cols = rings[k]
        for n in range(cols // step_w):
            c = pl.ds(at + n * step_w, step_w)
            pair_s[0, :, c] = jnp.dot(
                sel[1], ow[:, c], preferred_element_type=F32
            ).astype(BF16)
        pair_start(k)
    for n in range(width // step_w):
        c = pl.ds(n * step_w, step_w)
        keep[0, :, c] = jnp.dot(sel[0], ow[:, c], preferred_element_type=F32)
    for h in range(1, hops + 1):
        for k in first_rings:
            ring_step(k, h)

    loads["routes"].wait()
    loads["route_w"].wait()
    for k in range(TOP):
        for part in range(parts):
            c = pl.ds(part * LANES, LANES)
            table[pl.ds(k * parts + part, 1), :] = routes[pl.ds(k, 1), c].astype(F32)
            table[pl.ds((TOP + k) * parts + part, 1), :] = route_w[pl.ds(k, 1), c]
    columns[:, pl.ds(0, 2 * TOP * parts)] = table[...].T
    base = tp * rows
    my_part = lax.div(base, LANES)
    mine = columns[pl.ds(pl.multiple_of(base - my_part * LANES, rows), rows), :]

    def column(n):
        found = mine[:, n * parts : n * parts + 1]
        for part in range(1, parts):
            found = jnp.where(
                my_part == part, mine[:, n * parts + part : n * parts + part + 1], found
            )
        return found

    lane = lax.broadcasted_iota(jnp.int32, (rows, LANES), 1)
    pos = jnp.floor((lane.astype(F32) + 0.5) * (1.0 / cap)).astype(jnp.int32)
    depth = (lane - pos * cap).astype(F32)
    expert = jnp.where(lane < slots, pos, -1).astype(F32)
    first = (column(0) == expert).astype(F32)
    second = (column(1) == expert).astype(F32)
    named = first + second
    r_at = lax.broadcasted_iota(jnp.int32, (rows, rows), 0)
    c_at = lax.broadcasted_iota(jnp.int32, (rows, rows), 1)
    earlier = (c_at < r_at).astype(F32).astype(BF16)
    rank = jnp.dot(earlier, named.astype(BF16), preferred_element_type=F32)
    hit = named * (rank == depth).astype(F32)
    w_first, w_second = column(TOP), column(TOP + 1)
    w_sum = w_first + w_second
    mix_w = hit * (first * (w_first / w_sum) + second * (w_second / w_sum))
    pick = hit.T.astype(BF16)[:slots, :]

    loads["gains"].wait()
    loads["resid"].wait()
    gain_rows = gains[...]
    projected = jnp.concatenate([ring_end(k) for k in first_rings], axis=1)
    stream = resid[...].astype(F32) + rms_scale(projected, gain_rows[0:1, :])
    stream_ref[...] = stream
    normed = rms_scale(stream, gain_rows[1:2, :]).astype(BF16)

    outgoing = jnp.dot(pick, normed, preferred_element_type=F32)
    for b in range(folds):
        fold[pl.ds(b, slots, stride=folds), :] = outgoing[
            :, b * LANES : (b + 1) * LANES
        ]
    folded = fold[...].astype(BF16)
    zs[...] = folded
    my_piece = pl.ds(pl.multiple_of(sp * piece, piece), piece)
    zr[my_piece, :] = zs[my_piece, :]

    with jax.named_scope("above"):

        @pl.when(has_above)
        def _():
            pl.semaphore_wait(above_sem, n_sp - 1 - sp)

    for p in range(1, n_sp):
        d = (p + 1) // 2 if p % 2 else -(p // 2)
        there = lax.rem(sp + d + n_sp, n_sp)
        send(
            zs.at[pl.ds(pl.multiple_of(there * piece, piece), piece), :],
            zr.at[my_piece, :],
            z_send.at[0],
            z_recv.at[sp],
            {"sp": there},
        )

    gather = {}
    came = set()

    def block(cc, other, o):
        return pl.ds(cc * chunk_rows + other * own_rows + (o % chips) * TILE, TILE)

    part_w = width // 2

    def to_partner(cc, part, o):
        c = pl.ds(part * part_w, part_w)
        send(
            xbuf.at[block(cc, 0, o), c],
            xbuf.at[block(cc, 1, o), c],
            gather_send.at[0],
            d_recv.at[cc],
            partner,
        )

    def gather_hop(cc, part, h):
        with jax.named_scope(f"ag{cc}{part}{h}"):
            gather_step(cc, part, h)

    def arrive(src):
        @pl.when(sp != src)
        def _():
            settle(zr.at[pl.ds(src * piece, piece), :], z_recv.at[src])

    def gather_step(cc, part, h):
        if h == 1 and part == 0:
            for src in range(n_sp):
                if src not in came and src * piece < (cc + 1) * span:
                    came.add(src)
                    arrive(src)
            fold[pl.ds(cc * span, span), :] = zr[pl.ds(cc * span, span), :].astype(F32)
            for b in range(folds):
                xbuf[block(cc, 0, 0), pl.ds(b * LANES, LANES)] = fold[
                    pl.ds(cc * span + b, TILE, stride=folds), :
                ].astype(BF16)
        elif h > 1:
            gather[cc, part, "r", h - 1].wait_recv()
            gather[cc, part, "l", h - 1].wait_recv()
        k = cc * 2 + part
        for name, sign, dev, sem, half in (
            ("r", -1, right, ar_recv, 0),
            ("l", 1, left, al_recv, 1),
        ):
            c = pl.ds(part * part_w, part_w)
            if h == hops:
                c = pl.ds(part * part_w + half * (part_w // 2), part_w // 2)
            gather[cc, part, name, h] = send(
                xbuf.at[block(cc, 0, sign * (h - 1)), c],
                xbuf.at[block(cc, 0, sign * h), c],
                gather_send.at[0],
                sem.at[k, h - 1],
                dev,
            )
        to_partner(cc, part, 1 - h)
        if h > 1:
            to_partner(cc, part, h - 1)

    def gather_last(cc, part):
        with jax.named_scope(f"al{cc}{part}"):
            gather[cc, part, "r", hops].wait_recv()
            gather[cc, part, "l", hops].wait_recv()
            to_partner(cc, part, hops)

    def experts(cc):
        s = cc + 1
        with jax.named_scope(f"exw{cc}"):
            settle(
                xbuf.at[pl.ds(cc * chunk_rows + own_rows, own_rows), :], d_recv.at[cc]
            )
        with jax.named_scope(f"exc{cc}"):
            x = xbuf[pl.ds(cc * chunk_rows, chunk_rows), :]
            g = jnp.dot(x, wg[...], preferred_element_type=F32)
            u = jnp.dot(x, wu[...], preferred_element_type=F32)
            hid[...] = (g / (1.0 + jnp.exp(-g)) * u).astype(BF16)
            for n in range(width // step_w):
                c = pl.ds(n * step_w, step_w)
                pair_s[s, :, c] = jnp.dot(
                    hid[pl.ds(own_rows, own_rows), :],
                    wd[:, c],
                    preferred_element_type=F32,
                ).astype(BF16)
            for k in set_rings[s]:
                pair_start(k)
            for n in range(width // step_w):
                c = pl.ds(n * step_w, step_w)
                keep[s, :, c] = jnp.dot(
                    hid[pl.ds(0, own_rows), :], wd[:, c], preferred_element_type=F32
                )

    finished = set()
    back_sent = set()
    ended = {}

    def finish(cc, part):
        k = set_rings[cc + 1][part]
        total = ring_end(k)
        first_fold = rings[k][1] // LANES
        for b in range(rings[k][2] // LANES):
            fold[pl.ds(cc * span + first_fold + b, TILE, stride=folds), :] = total[
                :, b * LANES : (b + 1) * LANES
            ]
        ended[cc] = ended.get(cc, 0) + 1
        if ended[cc] < len(set_rings[cc + 1]):
            return
        at = pl.ds(cc * span, span)
        bs[at, :] = fold[at, :].astype(BF16)
        finished.add(cc)
        for p in range(n_sp):
            needs = {p * piece // span, ((p + 1) * piece - 1) // span}
            if p not in back_sent and needs <= finished:
                back_sent.add(p)

                @pl.when(sp != p)
                def _():
                    send(
                        bs.at[pl.ds(p * piece, piece), :],
                        br.at[my_piece, :],
                        z_send.at[1],
                        back_recv.at[0],
                        {"sp": p},
                    )

    for name in ("wg", "wu", "wd"):
        loads[name].wait()
    for op in ORDER:
        if op[0] == 0:
            gather_hop(*op[1:])
        elif op[0] == 4:
            gather_last(*op[1:])
        elif op[0] == 1:
            experts(*op[1:])
        elif op[0] == 2:
            ring_step(set_rings[op[1] + 1][op[2]], op[3])
        else:
            finish(*op[1:])
    br[my_piece, :] = bs[my_piece, :]

    far = (n_sp - 1) * piece
    ring_rows = (2 * hops - 1) * TILE
    with jax.named_scope("sendwait"):
        settle(pair_s, pair_send.at[0])
        settle(pair_s.at[:, pl.ds(0, ring_rows), :], ring_send.at[0])
        settle(
            xbuf.at[pl.ds(0, chunks * (ring_rows + own_rows)), :], gather_send.at[0]
        )
        settle(zs.at[pl.ds(piece, far), :], z_send.at[0])

        @pl.when(has_above)
        def _():
            halo.wait_send()

    with jax.named_scope("backwait"):
        settle(br.at[pl.ds(piece, far), :], back_recv.at[0])
    fold[...] = br[...].astype(F32)
    for b in range(folds):
        back[:, pl.ds(b * LANES, LANES)] = fold[
            pl.ds(b, slots, stride=folds), :
        ].astype(BF16)
    mix_w = mix_w[:, :slots]
    mix_hi = mix_w.astype(BF16)
    mix_lo = (mix_w - mix_hi.astype(F32)).astype(BF16)
    picked = back[...]
    combined = jnp.dot(mix_hi, picked, preferred_element_type=F32) + jnp.dot(
        mix_lo, picked, preferred_element_type=F32
    )
    out[...] = stream_ref[...] + rms_scale(combined, gain_rows[2:3, :])
    settle(bs.at[pl.ds(piece, far), :], z_send.at[1])


def per_device(
    resid,
    gate_b,
    gate_c,
    value,
    taps,
    doc_ids,
    out_weight,
    norm_gains,
    routes,
    route_weights,
    w_gate,
    w_up,
    w_down,
):
    n_sp, n_tp = lax.axis_size("sp"), lax.axis_size("tp")
    tok, ch = gate_b.shape
    rows, width = resid.shape
    units = w_gate.shape[2]
    cap = max(2, 3 * TOP * rows // (2 * n_sp))
    chips = n_tp // 2
    hops = chips // 2
    slots = n_sp * cap
    chunks = slots // TILE
    folds = width // LANES
    sets = chunks + 1
    own_rows = chips * TILE
    parts = tok // LANES
    rings = [(0, k * (width // 4), width // 4) for k in range(4)]
    for s in range(1, sets):
        rings += [(s, k * (width // 2), width // 2) for k in range(2)]
    n_rings = len(rings)
    operands = (
        resid,
        gate_b,
        gate_c,
        value,
        taps,
        doc_ids.reshape(parts, LANES),
        out_weight,
        norm_gains,
        routes.T,
        route_weights.T,
        w_gate,
        w_up,
        w_down,
    )
    hbm = pl.BlockSpec(memory_space=pl.ANY)
    vmem = pltpu.VMEM
    dma = pltpu.SemaphoreType.DMA
    result = pl.pallas_call(
        functools.partial(layer_kernel, n_sp, n_tp, cap, rings),
        out_shape=jax.ShapeDtypeStruct((rows, width), F32),
        in_specs=[hbm] * len(operands),
        out_specs=pl.BlockSpec(memory_space=vmem),
        scratch_shapes=[
            *[vmem(a.shape, a.dtype) for a in operands[:10]],
            *[vmem(a.shape[1:], a.dtype) for a in operands[10:]],
            vmem((tok + 8, ch), F32),
            vmem((tok + 8, LANES), F32),
            vmem((16, ch), F32),
            vmem((16, ch), F32),
            vmem((tok, ch), BF16),
            vmem((2, own_rows, ch), BF16),
            vmem((2 * TOP * parts, LANES), F32),
            vmem((LANES, LANES), F32),
            vmem((slots * folds, LANES), BF16),
            vmem((slots * folds, LANES), BF16),
            vmem((slots * folds, LANES), BF16),
            vmem((slots * folds, LANES), BF16),
            vmem((slots * folds, LANES), F32),
            vmem((chunks * n_tp * TILE, width), BF16),
            vmem((n_tp * TILE, units), BF16),
            vmem((sets, own_rows, width), BF16),
            vmem((sets, own_rows, width), BF16),
            vmem((sets, own_rows, width), F32),
            vmem((sets, chips, TILE, width), BF16),
            vmem((sets, hops, TILE, width), BF16),
            vmem((sets, hops, TILE, width), BF16),
            vmem((rows, width), F32),
            vmem((slots, width), BF16),
            dma((len(operands),)),
            dma((2,)),
            pltpu.SemaphoreType.REGULAR,
            pltpu.SemaphoreType.REGULAR,
            dma((2,)),
            dma((n_sp,)),
            dma((1,)),
            dma((1,)),
            dma((n_rings,)),
            dma((1,)),
            dma((n_rings, hops)),
            dma((n_rings, hops)),
            dma((1,)),
            dma((chunks,)),
            dma((chunks * 2, hops)),
            dma((chunks * 2, hops)),
        ],
        compiler_params=pltpu.CompilerParams(
            collective_id=0,
            has_side_effects=True,
            vmem_limit_bytes=56 * 1024 * 1024,
        ),
        name="layer",
    )(*operands)
    return result.astype(BF16)


def solution(mesh):
    return jax.shard_map(
        per_device,
        mesh=mesh,
        in_specs=(
            P(("grp", "sp", "tp"), None),
            P(("grp", "sp"), "tp"),
            P(("grp", "sp"), "tp"),
            P(("grp", "sp"), "tp"),
            P(None, "tp"),
            P(("grp", "sp")),
            P("tp", None),
            P(),
            P(("grp", "sp"), None),
            P(("grp", "sp"), None),
            P("sp", None, "tp"),
            P("sp", None, "tp"),
            P("sp", "tp", None),
        ),
        out_specs=P(("grp", "sp", "tp"), None),
        check_vma=False,
    )
```

```python
import functools

import jax
import jax.numpy as jnp
from jax import lax
from jax.experimental import pallas as pl
from jax.experimental.pallas import tpu as pltpu
from jax.sharding import PartitionSpec as P

TAPS = 3
TOP = 2
LANES = 128
TILE = 16

norm_eps = 1e-06

ORDER = (
    (0, 0, 0, 1), (0, 0, 1, 1), (0, 1, 0, 1), (0, 1, 1, 1), (0, 0, 0, 2),
    (0, 0, 1, 2), (0, 1, 0, 2), (0, 1, 1, 2), (0, 0, 0, 3), (0, 0, 1, 3),
    (0, 1, 0, 3), (0, 2, 0, 1), (0, 2, 1, 1), (0, 0, 0, 4), (0, 1, 1, 3),
    (0, 0, 1, 4), (0, 1, 0, 4), (0, 2, 0, 2), (0, 2, 1, 2), (4, 0, 0),
    (4, 0, 1), (4, 1, 0), (0, 2, 0, 3), (0, 2, 1, 3), (0, 1, 1, 4),
    (1, 0), (0, 2, 0, 4), (0, 2, 1, 4), (4, 1, 1), (2, 0, 0, 1),
    (2, 0, 1, 1), (4, 2, 0), (4, 2, 1), (2, 0, 0, 2), (2, 0, 1, 2),
    (1, 2), (1, 1), (2, 2, 0, 1), (2, 2, 1, 1), (2, 1, 0, 1),
    (2, 1, 1, 1), (2, 0, 0, 3), (2, 0, 1, 3), (2, 2, 0, 2), (2, 2, 1, 2),
    (2, 1, 0, 2), (2, 1, 1, 2), (2, 0, 0, 4), (2, 2, 0, 3), (2, 2, 1, 3),
    (2, 1, 0, 3), (2, 1, 1, 3), (3, 0, 0), (2, 2, 0, 4), (2, 2, 1, 4),
    (2, 1, 0, 4), (2, 1, 1, 4), (2, 0, 1, 4), (3, 2, 0), (3, 2, 1),
    (3, 1, 0), (3, 1, 1), (3, 0, 1),
)
BF16 = jnp.bfloat16
F32 = jnp.float32
MESH = pl.DeviceIdType.MESH


def rms_scale(values, gain_row):
    mean_sq = jnp.mean(values * values, axis=-1, keepdims=True)
    return values * lax.rsqrt(mean_sq + norm_eps) * gain_row


def layer_kernel(
    n_sp,
    n_tp,
    cap,
    rings,
    resid_h,
    gate_b_h,
    gate_c_h,
    value_h,
    taps_h,
    ids_h,
    out_w_h,
    gains_h,
    routes_h,
    route_w_h,
    w_gate_h,
    w_up_h,
    w_down_h,
    out,
    resid,
    gate_b,
    gate_c,
    value,
    taps,
    ids,
    ow,
    gains,
    routes,
    route_w,
    wg,
    wu,
    wd,
    ext,
    ext_ids,
    halo_s,
    halo_r,
    mixed,
    sel,
    table,
    columns,
    zs,
    zr,
    bs,
    br,
    fold,
    xbuf,
    hid,
    pair_s,
    pair_r,
    keep,
    ring_s,
    ring_r,
    ring_l,
    stream_ref,
    back,
    load_sem,
    halo_sem,
    below_sem,
    all_sem,
    z_send,
    z_recv,
    back_recv,
    pair_send,
    pair_recv,
    ring_send,
    r_recv,
    gather_send,
    d_recv,
    a_recv,
):
    tok, ch = gate_b.shape
    rows, width = resid.shape
    chips = n_tp // 2
    hops = chips // 2
    folds = width // LANES
    slots = n_sp * cap
    chunks = slots // TILE
    chunk_rows = n_tp * TILE
    own_rows = chips * TILE
    piece = cap * folds
    span = TILE * folds

    tp = lax.axis_index("tp")
    sp = lax.axis_index("sp")
    core = lax.rem(tp, 2)
    chip = lax.div(tp, 2)
    partner = {"tp": chip * 2 + (1 - core)}
    right = {"tp": lax.rem(chip + 1, chips) * 2 + core}
    left = {"tp": lax.rem(chip + chips - 1, chips) * 2 + core}

    def along(d):
        return {"sp": lax.rem(sp + d + n_sp, n_sp)}

    def remote(src, dst, s_sem, r_sem, dev):
        return pltpu.make_async_remote_copy(
            src_ref=src,
            dst_ref=dst,
            send_sem=s_sem,
            recv_sem=r_sem,
            device_id=dev,
            device_id_type=MESH,
        )

    def send(src, dst, s_sem, r_sem, dev):
        copy = remote(src, dst, s_sem, r_sem, dev)
        copy.start()
        return copy

    def settle(ref, sem):
        pltpu.make_async_copy(ref, ref, sem).wait()

    barrier = pltpu.get_barrier_semaphore()
    greeted = [partner, right, left, along(-1), along(1)]
    for dev in greeted:
        pl.semaphore_signal(barrier, inc=1, device_id=dev, device_id_type=MESH)
    last = n_sp - 1
    has_below, has_above = sp > 0, sp < last

    loads = {}
    for i, (name, src, dst) in enumerate(
        (
            ("ids", ids_h, ids),
            ("gate_c", gate_c_h, gate_c),
            ("value", value_h, value),
            ("gate_b", gate_b_h, gate_b),
            ("taps", taps_h, taps),
            ("ow", out_w_h, ow),
            ("routes", routes_h, routes),
            ("route_w", route_w_h, route_w),
            ("gains", gains_h, gains),
            ("resid", resid_h, resid),
            ("wg", w_gate_h.at[0], wg),
            ("wu", w_up_h.at[0], wu),
            ("wd", w_down_h.at[0], wd),
        )
    ):
        loads[name] = pltpu.make_async_copy(src, dst, load_sem.at[i])
        loads[name].start()

    parts = tok // LANES
    loads["ids"].wait()
    for k in range(parts):
        line = ids[k : k + 1, :].astype(F32)
        ext_ids[pl.ds(8 + k * LANES, LANES), :] = jnp.broadcast_to(
            line, (LANES, LANES)
        ).T
    loads["gate_c"].wait()
    loads["value"].wait()
    product = gate_c[...].astype(F32) * value[...].astype(F32)
    ext[pl.ds(8, tok), :] = product
    halo_s[pl.ds(0, 8), :] = product[tok - 8 :]
    halo_s[pl.ds(8, 8), :] = ext_ids[pl.ds(tok, 8), :]

    with jax.named_scope("barrier"):
        pl.semaphore_wait(barrier, len(greeted))
    halo = remote(halo_s, halo_r, halo_sem.at[0], halo_sem.at[1], along(1))

    @pl.when(has_above)
    def _():
        halo.start()

    with jax.named_scope("chain"):

        @pl.when(sp > 2)
        def _():
            pl.semaphore_wait(below_sem, 1)

        @pl.when((sp >= 2) & has_above)
        def _():
            pl.semaphore_signal(
                below_sem, inc=1, device_id=along(1), device_id_type=MESH
            )

        @pl.when(sp == 0)
        def _():
            pl.semaphore_signal(
                all_sem, inc=1, device_id=along(-1), device_id_type=MESH
            )

    ext[pl.ds(0, 8), :] = jnp.zeros((8, ch), F32)
    ext_ids[pl.ds(0, 8), :] = jnp.full((8, LANES), -1.0, F32)
    loads["gate_b"].wait()
    loads["taps"].wait()

    @pl.when(has_below)
    def _():
        halo.wait_recv()
        ext[pl.ds(0, 8), :] = halo_r[pl.ds(0, 8), :]
        ext_ids[pl.ds(0, 8), :] = halo_r[pl.ds(8, 8), :]

    here = ext_ids[pl.ds(8, tok), :]
    tap_rows = taps[...].astype(F32)
    conv = tap_rows[0:1, :] * ext[pl.ds(8, tok), :]
    for lag in range(1, TAPS):
        same = ext_ids[pl.ds(8 - lag, tok), :] == here
        conv = conv + jnp.where(
            same, tap_rows[lag : lag + 1, :] * ext[pl.ds(8 - lag, tok), :], 0.0
        )
    mixed[...] = (gate_b[...].astype(F32) * conv).astype(BF16)

    def place(owner, o):
        block = lax.rem(chip + o, chips) * 2 + owner
        return pl.ds(pl.multiple_of(block * rows, rows), rows)

    for o in range(chips):
        sel[0, pl.ds(o * rows, rows), :] = mixed[place(core, o), :]
        sel[1, pl.ds(o * rows, rows), :] = mixed[place(1 - core, o), :]

    ring = {}

    def pair_start(k):
        s, at, cols = rings[k]
        at = pl.ds(at, cols)
        ring[k, "pair"] = send(
            pair_s.at[s, :, at],
            pair_r.at[s, :, at],
            pair_send.at[0],
            pair_recv.at[k],
            partner,
        )

    def hop_wait(k, h):
        _, at, cols = rings[k]
        settle(
            pair_r.at[0, pl.ds(0, TILE if h == 1 else 2 * TILE), pl.ds(at, cols)],
            r_recv.at[k, h - 1],
        )

    def ring_step(k, h):
        with jax.named_scope(f"rs{k}_{h}"):
            ring_hop(k, h)

    def ring_hop(k, h):
        s, at, cols = rings[k]
        all_c = pl.ds(at, cols)
        lo, hi = pl.ds(at, cols // 2), pl.ds(at + cols // 2, cols // 2)

        def share(o, c):
            r = pl.ds(o * TILE, TILE)
            return keep[s, r, c] + pair_r[s, r, c].astype(F32)

        if h == 1:
            ring[k, "pair"].wait_recv()
            ring_s[s, hops, :, all_c] = share(hops, all_c).astype(BF16)
        else:
            hop_wait(k, h - 1)
        for buf, dev, early, late, o in (
            (ring_r, right, lo, hi, hops + 1 - h),
            (ring_l, left, hi, lo, (chips - hops - 1 + h) % chips),
        ):
            if h == 2:
                ring_s[s, o, :, early] = (
                    share(o, early) + buf[s, 0, :, early].astype(F32)
                ).astype(BF16)
                ring_s[s, o, :, late] = share(o, late).astype(BF16)
            elif h > 2:
                ring_s[s, o, :, all_c] = (
                    share(o, all_c) + buf[s, h - 2, :, all_c].astype(F32)
                ).astype(BF16)
            c = early if h == 1 else all_c
            send(
                ring_s.at[s, o, :, c],
                buf.at[s, h - 1, :, c],
                ring_send.at[0],
                r_recv.at[k, h - 1],
                dev,
            )

    def ring_end(k):
        with jax.named_scope(f"re{k}"):
            s, at, cols = rings[k]
            c = pl.ds(at, cols)
            hop_wait(k, hops)
            return (
                keep[s, pl.ds(0, TILE), c]
                + pair_r[s, pl.ds(0, TILE), c].astype(F32)
                + ring_r[s, hops - 1, :, c].astype(F32)
                + ring_l[s, hops - 1, :, c].astype(F32)
            )

    set_rings = {}
    for k, (s, _, _) in enumerate(rings):
        set_rings.setdefault(s, []).append(k)
    first_rings = set_rings[0]
    loads["ow"].wait()
    step_w = min(512, width)
    for k in first_rings:
        _, at, cols = rings[k]
        for n in range(cols // step_w):
            c = pl.ds(at + n * step_w, step_w)
            pair_s[0, :, c] = jnp.dot(
                sel[1], ow[:, c], preferred_element_type=F32
            ).astype(BF16)
        pair_start(k)
    @pl.when(sp == last)
    def _():
        pl.semaphore_wait(all_sem, 1)
        for there in range(last):
            pl.semaphore_signal(
                all_sem, inc=1, device_id={"sp": there}, device_id_type=MESH
            )

    for n in range(width // step_w):
        c = pl.ds(n * step_w, step_w)
        keep[0, :, c] = jnp.dot(sel[0], ow[:, c], preferred_element_type=F32)
    for h in range(1, hops + 1):
        for k in first_rings:
            ring_step(k, h)

    loads["routes"].wait()
    loads["route_w"].wait()
    for k in range(TOP):
        for part in range(parts):
            c = pl.ds(part * LANES, LANES)
            table[pl.ds(k * parts + part, 1), :] = routes[pl.ds(k, 1), c].astype(F32)
            table[pl.ds((TOP + k) * parts + part, 1), :] = route_w[pl.ds(k, 1), c]
    columns[:, pl.ds(0, 2 * TOP * parts)] = table[...].T
    base = tp * rows
    my_part = lax.div(base, LANES)
    mine = columns[pl.ds(pl.multiple_of(base - my_part * LANES, rows), rows), :]

    def column(n):
        found = mine[:, n * parts : n * parts + 1]
        for part in range(1, parts):
            found = jnp.where(
                my_part == part, mine[:, n * parts + part : n * parts + part + 1], found
            )
        return found

    lane = lax.broadcasted_iota(jnp.int32, (rows, LANES), 1)
    pos = jnp.floor((lane.astype(F32) + 0.5) * (1.0 / cap)).astype(jnp.int32)
    depth = (lane - pos * cap).astype(F32)
    expert = jnp.where(lane < slots, pos, -1).astype(F32)
    first = (column(0) == expert).astype(F32)
    second = (column(1) == expert).astype(F32)
    named = first + second
    r_at = lax.broadcasted_iota(jnp.int32, (rows, rows), 0)
    c_at = lax.broadcasted_iota(jnp.int32, (rows, rows), 1)
    earlier = (c_at < r_at).astype(F32).astype(BF16)
    rank = jnp.dot(earlier, named.astype(BF16), preferred_element_type=F32)
    hit = named * (rank == depth).astype(F32)
    w_first, w_second = column(TOP), column(TOP + 1)
    w_sum = w_first + w_second
    mix_w = hit * (first * (w_first / w_sum) + second * (w_second / w_sum))
    pick = hit.T.astype(BF16)[:slots, :]

    loads["gains"].wait()
    loads["resid"].wait()
    gain_rows = gains[...]
    projected = jnp.concatenate([ring_end(k) for k in first_rings], axis=1)
    stream = resid[...].astype(F32) + rms_scale(projected, gain_rows[0:1, :])
    stream_ref[...] = stream
    normed = rms_scale(stream, gain_rows[1:2, :]).astype(BF16)

    outgoing = jnp.dot(pick, normed, preferred_element_type=F32)
    for b in range(folds):
        fold[pl.ds(b, slots, stride=folds), :] = outgoing[
            :, b * LANES : (b + 1) * LANES
        ]
    folded = fold[...].astype(BF16)
    zs[...] = folded
    my_piece = pl.ds(pl.multiple_of(sp * piece, piece), piece)
    zr[my_piece, :] = zs[my_piece, :]

    with jax.named_scope("above"):

        @pl.when(has_above)
        def _():
            pl.semaphore_wait(all_sem, 1)

    for p in range(1, n_sp):
        d = (p + 1) // 2 if p % 2 else -(p // 2)
        there = lax.rem(sp + d + n_sp, n_sp)
        send(
            zs.at[pl.ds(pl.multiple_of(there * piece, piece), piece), :],
            zr.at[my_piece, :],
            z_send.at[0],
            z_recv.at[sp],
            {"sp": there},
        )

    came = set()

    def block(cc, other, o):
        return pl.ds(cc * chunk_rows + other * own_rows + (o % chips) * TILE, TILE)

    part_w = width // 2

    def to_partner(cc, part, o):
        c = pl.ds(part * part_w, part_w)
        send(
            xbuf.at[block(cc, 0, o), c],
            xbuf.at[block(cc, 1, o), c],
            gather_send.at[0],
            d_recv.at[cc],
            partner,
        )

    def gather_hop(cc, part, h):
        with jax.named_scope(f"ag{cc}{part}{h}"):
            gather_step(cc, part, h)

    def arrive(src):
        @pl.when(sp != src)
        def _():
            settle(zr.at[pl.ds(src * piece, piece), :], z_recv.at[src])

    def gather_step(cc, part, h):
        if h == 1 and part == 0:
            for src in range(n_sp):
                if src not in came and src * piece < (cc + 1) * span:
                    came.add(src)
                    arrive(src)
            fold[pl.ds(cc * span, span), :] = zr[pl.ds(cc * span, span), :].astype(F32)
            for b in range(folds):
                xbuf[block(cc, 0, 0), pl.ds(b * LANES, LANES)] = fold[
                    pl.ds(cc * span + b, TILE, stride=folds), :
                ].astype(BF16)
        elif h > 1:
            settle(
                xbuf.at[pl.ds(0, 2 * TILE), pl.ds(0, part_w)],
                a_recv.at[cc * 2 + part, h - 2],
            )
        for sign, dev, half in ((-1, right, 0), (1, left, 1)):
            c = pl.ds(part * part_w, part_w)
            if h == hops:
                c = pl.ds(part * part_w + half * (part_w // 2), part_w // 2)
            send(
                xbuf.at[block(cc, 0, sign * (h - 1)), c],
                xbuf.at[block(cc, 0, sign * h), c],
                gather_send.at[0],
                a_recv.at[cc * 2 + part, h - 1],
                dev,
            )
        to_partner(cc, part, 1 - h)
        if h > 1:
            to_partner(cc, part, h - 1)

    def gather_last(cc, part):
        with jax.named_scope(f"al{cc}{part}"):
            settle(
                xbuf.at[pl.ds(0, TILE), pl.ds(0, part_w)],
                a_recv.at[cc * 2 + part, hops - 1],
            )
            to_partner(cc, part, hops)

    def experts(cc):
        s = cc + 1
        with jax.named_scope(f"exw{cc}"):
            settle(
                xbuf.at[pl.ds(cc * chunk_rows + own_rows, own_rows), :], d_recv.at[cc]
            )
        with jax.named_scope(f"exc{cc}"):
            x = xbuf[pl.ds(cc * chunk_rows, chunk_rows), :]
            g = jnp.dot(x, wg[...], preferred_element_type=F32)
            u = jnp.dot(x, wu[...], preferred_element_type=F32)
            hid[...] = (g / (1.0 + jnp.exp(-g)) * u).astype(BF16)
            for n in range(width // step_w):
                c = pl.ds(n * step_w, step_w)
                pair_s[s, :, c] = jnp.dot(
                    hid[pl.ds(own_rows, own_rows), :],
                    wd[:, c],
                    preferred_element_type=F32,
                ).astype(BF16)
            for k in set_rings[s]:
                pair_start(k)
            for n in range(width // step_w):
                c = pl.ds(n * step_w, step_w)
                keep[s, :, c] = jnp.dot(
                    hid[pl.ds(0, own_rows), :], wd[:, c], preferred_element_type=F32
                )

    finished = set()
    back_sent = set()
    ended = {}

    def finish(cc, part):
        k = set_rings[cc + 1][part]
        total = ring_end(k)
        first_fold = rings[k][1] // LANES
        for b in range(rings[k][2] // LANES):
            fold[pl.ds(cc * span + first_fold + b, TILE, stride=folds), :] = total[
                :, b * LANES : (b + 1) * LANES
            ]
        ended[cc] = ended.get(cc, 0) + 1
        if ended[cc] < len(set_rings[cc + 1]):
            return
        at = pl.ds(cc * span, span)
        bs[at, :] = fold[at, :].astype(BF16)
        finished.add(cc)
        for p in range(n_sp):
            needs = {p * piece // span, ((p + 1) * piece - 1) // span}
            if p not in back_sent and needs <= finished:
                back_sent.add(p)

                @pl.when(sp != p)
                def _():
                    send(
                        bs.at[pl.ds(p * piece, piece), :],
                        br.at[my_piece, :],
                        z_send.at[1],
                        back_recv.at[0],
                        {"sp": p},
                    )

    for name in ("wg", "wu", "wd"):
        loads[name].wait()
    for op in ORDER:
        if op[0] == 0:
            gather_hop(*op[1:])
        elif op[0] == 4:
            gather_last(*op[1:])
        elif op[0] == 1:
            experts(*op[1:])
        elif op[0] == 2:
            ring_step(set_rings[op[1] + 1][op[2]], op[3])
        else:
            finish(*op[1:])
    br[my_piece, :] = bs[my_piece, :]

    far = (n_sp - 1) * piece
    ring_rows = (2 * hops - 1) * TILE
    with jax.named_scope("sendwait"):
        settle(pair_s, pair_send.at[0])
        settle(pair_s.at[:, pl.ds(0, ring_rows), :], ring_send.at[0])
        settle(
            xbuf.at[pl.ds(0, chunks * (ring_rows + own_rows)), :], gather_send.at[0]
        )
        settle(zs.at[pl.ds(piece, far), :], z_send.at[0])

        @pl.when(has_above)
        def _():
            halo.wait_send()

    with jax.named_scope("backwait"):
        settle(br.at[pl.ds(piece, far), :], back_recv.at[0])
    fold[...] = br[...].astype(F32)
    for b in range(folds):
        back[:, pl.ds(b * LANES, LANES)] = fold[
            pl.ds(b, slots, stride=folds), :
        ].astype(BF16)
    mix_w = mix_w[:, :slots]
    mix_hi = mix_w.astype(BF16)
    mix_lo = (mix_w - mix_hi.astype(F32)).astype(BF16)
    picked = back[...]
    combined = jnp.dot(mix_hi, picked, preferred_element_type=F32) + jnp.dot(
        mix_lo, picked, preferred_element_type=F32
    )
    out[...] = stream_ref[...] + rms_scale(combined, gain_rows[2:3, :])
    settle(bs.at[pl.ds(piece, far), :], z_send.at[1])


def per_device(
    resid,
    gate_b,
    gate_c,
    value,
    taps,
    doc_ids,
    out_weight,
    norm_gains,
    routes,
    route_weights,
    w_gate,
    w_up,
    w_down,
):
    n_sp, n_tp = lax.axis_size("sp"), lax.axis_size("tp")
    tok, ch = gate_b.shape
    rows, width = resid.shape
    units = w_gate.shape[2]
    cap = max(2, 3 * TOP * rows // (2 * n_sp))
    chips = n_tp // 2
    hops = chips // 2
    slots = n_sp * cap
    chunks = slots // TILE
    folds = width // LANES
    sets = chunks + 1
    own_rows = chips * TILE
    parts = tok // LANES
    rings = [(0, k * (width // 4), width // 4) for k in range(4)]
    for s in range(1, sets):
        rings += [(s, k * (width // 2), width // 2) for k in range(2)]
    n_rings = len(rings)
    operands = (
        resid,
        gate_b,
        gate_c,
        value,
        taps,
        doc_ids.reshape(parts, LANES),
        out_weight,
        norm_gains,
        routes.T,
        route_weights.T,
        w_gate,
        w_up,
        w_down,
    )
    hbm = pl.BlockSpec(memory_space=pl.ANY)
    vmem = pltpu.VMEM
    dma = pltpu.SemaphoreType.DMA
    result = pl.pallas_call(
        functools.partial(layer_kernel, n_sp, n_tp, cap, rings),
        out_shape=jax.ShapeDtypeStruct((rows, width), F32),
        in_specs=[hbm] * len(operands),
        out_specs=pl.BlockSpec(memory_space=vmem),
        scratch_shapes=[
            *[vmem(a.shape, a.dtype) for a in operands[:10]],
            *[vmem(a.shape[1:], a.dtype) for a in operands[10:]],
            vmem((tok + 8, ch), F32),
            vmem((tok + 8, LANES), F32),
            vmem((16, ch), F32),
            vmem((16, ch), F32),
            vmem((tok, ch), BF16),
            vmem((2, own_rows, ch), BF16),
            vmem((2 * TOP * parts, LANES), F32),
            vmem((LANES, LANES), F32),
            vmem((slots * folds, LANES), BF16),
            vmem((slots * folds, LANES), BF16),
            vmem((slots * folds, LANES), BF16),
            vmem((slots * folds, LANES), BF16),
            vmem((slots * folds, LANES), F32),
            vmem((chunks * n_tp * TILE, width), BF16),
            vmem((n_tp * TILE, units), BF16),
            vmem((sets, own_rows, width), BF16),
            vmem((sets, own_rows, width), BF16),
            vmem((sets, own_rows, width), F32),
            vmem((sets, chips, TILE, width), BF16),
            vmem((sets, hops, TILE, width), BF16),
            vmem((sets, hops, TILE, width), BF16),
            vmem((rows, width), F32),
            vmem((slots, width), BF16),
            dma((len(operands),)),
            dma((2,)),
            pltpu.SemaphoreType.REGULAR,
            pltpu.SemaphoreType.REGULAR,
            dma((2,)),
            dma((n_sp,)),
            dma((1,)),
            dma((1,)),
            dma((n_rings,)),
            dma((1,)),
            dma((n_rings, hops)),
            dma((1,)),
            dma((chunks,)),
            dma((chunks * 2, hops)),
        ],
        compiler_params=pltpu.CompilerParams(
            collective_id=0,
            has_side_effects=True,
            vmem_limit_bytes=56 * 1024 * 1024,
        ),
        name="layer",
    )(*operands)
    return result.astype(BF16)


def solution(mesh):
    return jax.shard_map(
        per_device,
        mesh=mesh,
        in_specs=(
            P(("grp", "sp", "tp"), None),
            P(("grp", "sp"), "tp"),
            P(("grp", "sp"), "tp"),
            P(("grp", "sp"), "tp"),
            P(None, "tp"),
            P(("grp", "sp")),
            P("tp", None),
            P(),
            P(("grp", "sp"), None),
            P(("grp", "sp"), None),
            P("sp", None, "tp"),
            P("sp", None, "tp"),
            P("sp", "tp", None),
        ),
        out_specs=P(("grp", "sp", "tp"), None),
        check_vma=False,
    )
```

```python
import functools

import jax
import jax.numpy as jnp
from jax import lax
from jax.experimental import pallas as pl
from jax.experimental.pallas import tpu as pltpu
from jax.sharding import PartitionSpec as P

TAPS = 3
TOP = 2
LANES = 128
TILE = 16

norm_eps = 1e-06

ORDER = (
    (0, 0, 0, 1), (0, 0, 1, 1), (0, 1, 0, 1), (0, 1, 1, 1), (0, 0, 0, 2),
    (0, 0, 1, 2), (0, 1, 0, 2), (0, 1, 1, 2), (0, 0, 0, 3), (0, 0, 1, 3),
    (0, 1, 0, 3), (0, 2, 0, 1), (0, 2, 1, 1), (0, 1, 1, 3), (0, 0, 0, 4),
    (0, 0, 1, 4), (0, 1, 0, 4), (0, 2, 0, 2), (0, 2, 1, 2), (0, 1, 1, 4),
    (4, 0, 0), (4, 0, 1), (4, 1, 0), (0, 2, 0, 3), (0, 2, 1, 3),
    (4, 1, 1), (1, 0), (1, 1), (0, 2, 0, 4), (0, 2, 1, 4),
    (2, 0, 0, 1), (2, 0, 1, 1), (2, 1, 0, 1), (2, 1, 1, 1), (4, 2, 0),
    (4, 2, 1), (1, 2), (2, 1, 0, 2), (2, 2, 0, 1), (2, 2, 1, 1),
    (2, 1, 1, 2), (2, 0, 0, 2), (2, 0, 1, 2), (2, 2, 0, 2), (2, 2, 1, 2),
    (2, 1, 0, 3), (2, 1, 1, 3), (2, 0, 0, 3), (2, 2, 0, 3), (2, 2, 1, 3),
    (2, 0, 1, 3), (2, 1, 0, 4), (2, 1, 1, 4), (2, 2, 0, 4), (2, 2, 1, 4),
    (2, 0, 0, 4), (2, 0, 1, 4), (3, 1, 0), (3, 1, 1), (3, 2, 0),
    (3, 2, 1), (3, 0, 0), (3, 0, 1),
)
BF16 = jnp.bfloat16
F32 = jnp.float32
MESH = pl.DeviceIdType.MESH


def rms_scale(values, gain_row):
    mean_sq = jnp.mean(values * values, axis=-1, keepdims=True)
    return values * lax.rsqrt(mean_sq + norm_eps) * gain_row


def layer_kernel(
    n_sp,
    n_tp,
    cap,
    rings,
    resid_h,
    gate_b_h,
    gate_c_h,
    value_h,
    taps_h,
    ids_h,
    out_w_h,
    gains_h,
    routes_h,
    route_w_h,
    w_gate_h,
    w_up_h,
    w_down_h,
    out,
    resid,
    gate_b,
    gate_c,
    value,
    taps,
    ids,
    ow,
    gains,
    routes,
    route_w,
    wg,
    wu,
    wd,
    ext,
    ext_ids,
    halo_s,
    halo_r,
    mixed,
    sel,
    table,
    columns,
    zs,
    zr,
    bs,
    br,
    fold,
    xbuf,
    hid,
    pair_s,
    pair_r,
    keep,
    ring_s,
    ring_r,
    ring_l,
    stream_ref,
    back,
    load_sem,
    halo_sem,
    below_sem,
    all_sem,
    z_send,
    z_recv,
    back_recv,
    pair_send,
    pair_recv,
    ring_send,
    r_recv,
    gather_send,
    d_recv,
    a_recv,
):
    tok, ch = gate_b.shape
    rows, width = resid.shape
    chips = n_tp // 2
    hops = chips // 2
    folds = width // LANES
    slots = n_sp * cap
    chunks = slots // TILE
    chunk_rows = n_tp * TILE
    own_rows = chips * TILE
    piece = cap * folds
    span = TILE * folds

    tp = lax.axis_index("tp")
    sp = lax.axis_index("sp")
    core = lax.rem(tp, 2)
    chip = lax.div(tp, 2)
    partner = {"tp": chip * 2 + (1 - core)}
    right = {"tp": lax.rem(chip + 1, chips) * 2 + core}
    left = {"tp": lax.rem(chip + chips - 1, chips) * 2 + core}

    def along(d):
        return {"sp": lax.rem(sp + d + n_sp, n_sp)}

    def remote(src, dst, s_sem, r_sem, dev):
        return pltpu.make_async_remote_copy(
            src_ref=src,
            dst_ref=dst,
            send_sem=s_sem,
            recv_sem=r_sem,
            device_id=dev,
            device_id_type=MESH,
        )

    def send(src, dst, s_sem, r_sem, dev):
        copy = remote(src, dst, s_sem, r_sem, dev)
        copy.start()
        return copy

    def settle(ref, sem):
        pltpu.make_async_copy(ref, ref, sem).wait()

    barrier = pltpu.get_barrier_semaphore()
    greeted = [partner, right, left, along(-1), along(1)]
    for dev in greeted:
        pl.semaphore_signal(barrier, inc=1, device_id=dev, device_id_type=MESH)
    last = n_sp - 1
    has_below, has_above = sp > 0, sp < last

    loads = {}
    for i, (name, src, dst) in enumerate(
        (
            ("ids", ids_h, ids),
            ("gate_c", gate_c_h, gate_c),
            ("value", value_h, value),
            ("gate_b", gate_b_h, gate_b),
            ("taps", taps_h, taps),
            ("ow", out_w_h, ow),
            ("routes", routes_h, routes),
            ("route_w", route_w_h, route_w),
            ("gains", gains_h, gains),
            ("resid", resid_h, resid),
            ("wg", w_gate_h.at[0], wg),
            ("wu", w_up_h.at[0], wu),
            ("wd", w_down_h.at[0], wd),
        )
    ):
        loads[name] = pltpu.make_async_copy(src, dst, load_sem.at[i])
        loads[name].start()

    parts = tok // LANES
    loads["ids"].wait()
    for k in range(parts):
        line = ids[k : k + 1, :].astype(F32)
        ext_ids[pl.ds(8 + k * LANES, LANES), :] = jnp.broadcast_to(
            line, (LANES, LANES)
        ).T
    loads["gate_c"].wait()
    loads["value"].wait()
    product = gate_c[...].astype(F32) * value[...].astype(F32)
    ext[pl.ds(8, tok), :] = product
    halo_s[pl.ds(0, 8), :] = product[tok - 8 :]
    halo_s[pl.ds(8, 8), :] = ext_ids[pl.ds(tok, 8), :]

    with jax.named_scope("barrier"):
        pl.semaphore_wait(barrier, len(greeted))
    halo = remote(halo_s, halo_r, halo_sem.at[0], halo_sem.at[1], along(1))

    @pl.when(has_above)
    def _():
        halo.start()

    with jax.named_scope("chain"):

        @pl.when(sp > 2)
        def _():
            pl.semaphore_wait(below_sem, 1)

        @pl.when((sp >= 2) & has_above)
        def _():
            pl.semaphore_signal(
                below_sem, inc=1, device_id=along(1), device_id_type=MESH
            )

        @pl.when(sp == 0)
        def _():
            pl.semaphore_signal(
                all_sem, inc=1, device_id=along(-1), device_id_type=MESH
            )

    ext[pl.ds(0, 8), :] = jnp.zeros((8, ch), F32)
    ext_ids[pl.ds(0, 8), :] = jnp.full((8, LANES), -1.0, F32)
    loads["gate_b"].wait()
    loads["taps"].wait()

    @pl.when(has_below)
    def _():
        halo.wait_recv()
        ext[pl.ds(0, 8), :] = halo_r[pl.ds(0, 8), :]
        ext_ids[pl.ds(0, 8), :] = halo_r[pl.ds(8, 8), :]

    here = ext_ids[pl.ds(8, tok), :]
    tap_rows = taps[...].astype(F32)
    conv = tap_rows[0:1, :] * ext[pl.ds(8, tok), :]
    for lag in range(1, TAPS):
        same = ext_ids[pl.ds(8 - lag, tok), :] == here
        conv = conv + jnp.where(
            same, tap_rows[lag : lag + 1, :] * ext[pl.ds(8 - lag, tok), :], 0.0
        )
    mixed[...] = (gate_b[...].astype(F32) * conv).astype(BF16)

    def place(owner, o):
        block = lax.rem(chip + o, chips) * 2 + owner
        return pl.ds(pl.multiple_of(block * rows, rows), rows)

    for o in range(chips):
        sel[0, pl.ds(o * rows, rows), :] = mixed[place(core, o), :]
        sel[1, pl.ds(o * rows, rows), :] = mixed[place(1 - core, o), :]

    ring = {}

    def pair_start(k):
        s, at, cols = rings[k]
        at = pl.ds(at, cols)
        ring[k, "pair"] = send(
            pair_s.at[s, :, at],
            pair_r.at[s, :, at],
            pair_send.at[0],
            pair_recv.at[k],
            partner,
        )

    def hop_wait(k, h):
        _, at, cols = rings[k]
        settle(
            pair_r.at[0, pl.ds(0, TILE if h == 1 else 2 * TILE), pl.ds(at, cols)],
            r_recv.at[k, h - 1],
        )

    def ring_step(k, h):
        with jax.named_scope(f"rs{k}_{h}"):
            ring_hop(k, h)

    def ring_hop(k, h):
        s, at, cols = rings[k]
        all_c = pl.ds(at, cols)
        lo, hi = pl.ds(at, cols // 2), pl.ds(at + cols // 2, cols // 2)

        def share(o, c):
            r = pl.ds(o * TILE, TILE)
            return keep[s, r, c] + pair_r[s, r, c].astype(F32)

        if h == 1:
            ring[k, "pair"].wait_recv()
            ring_s[s, hops, :, all_c] = share(hops, all_c).astype(BF16)
        else:
            hop_wait(k, h - 1)
        for buf, dev, early, late, o in (
            (ring_r, right, lo, hi, hops + 1 - h),
            (ring_l, left, hi, lo, (chips - hops - 1 + h) % chips),
        ):
            if h == 2:
                ring_s[s, o, :, early] = (
                    share(o, early) + buf[s, 0, :, early].astype(F32)
                ).astype(BF16)
                ring_s[s, o, :, late] = share(o, late).astype(BF16)
            elif h > 2:
                ring_s[s, o, :, all_c] = (
                    share(o, all_c) + buf[s, h - 2, :, all_c].astype(F32)
                ).astype(BF16)
            c = early if h == 1 else all_c
            send(
                ring_s.at[s, o, :, c],
                buf.at[s, h - 1, :, c],
                ring_send.at[0],
                r_recv.at[k, h - 1],
                dev,
            )

    def ring_end(k):
        with jax.named_scope(f"re{k}"):
            s, at, cols = rings[k]
            c = pl.ds(at, cols)
            hop_wait(k, hops)
            return (
                keep[s, pl.ds(0, TILE), c]
                + pair_r[s, pl.ds(0, TILE), c].astype(F32)
                + ring_r[s, hops - 1, :, c].astype(F32)
                + ring_l[s, hops - 1, :, c].astype(F32)
            )

    set_rings = {}
    for k, (s, _, _) in enumerate(rings):
        set_rings.setdefault(s, []).append(k)
    first_rings = set_rings[0]
    loads["ow"].wait()
    step_w = min(512, width)
    for k in first_rings:
        _, at, cols = rings[k]
        for n in range(cols // step_w):
            c = pl.ds(at + n * step_w, step_w)
            pair_s[0, :, c] = jnp.dot(
                sel[1], ow[:, c], preferred_element_type=F32
            ).astype(BF16)
        pair_start(k)
    @pl.when(sp == last)
    def _():
        pl.semaphore_wait(all_sem, 1)
        for there in range(last):
            pl.semaphore_signal(
                all_sem, inc=1, device_id={"sp": there}, device_id_type=MESH
            )

    for n in range(width // step_w):
        c = pl.ds(n * step_w, step_w)
        keep[0, :, c] = jnp.dot(sel[0], ow[:, c], preferred_element_type=F32)
    for h in range(1, hops + 1):
        for k in first_rings:
            ring_step(k, h)

    loads["routes"].wait()
    loads["route_w"].wait()
    for k in range(TOP):
        for part in range(parts):
            c = pl.ds(part * LANES, LANES)
            table[pl.ds(k * parts + part, 1), :] = routes[pl.ds(k, 1), c].astype(F32)
            table[pl.ds((TOP + k) * parts + part, 1), :] = route_w[pl.ds(k, 1), c]
    columns[:, pl.ds(0, 2 * TOP * parts)] = table[...].T
    base = tp * rows
    my_part = lax.div(base, LANES)
    mine = columns[pl.ds(pl.multiple_of(base - my_part * LANES, rows), rows), :]

    def column(n):
        found = mine[:, n * parts : n * parts + 1]
        for part in range(1, parts):
            found = jnp.where(
                my_part == part, mine[:, n * parts + part : n * parts + part + 1], found
            )
        return found

    lane = lax.broadcasted_iota(jnp.int32, (rows, LANES), 1)
    pos = jnp.floor((lane.astype(F32) + 0.5) * (1.0 / cap)).astype(jnp.int32)
    depth = (lane - pos * cap).astype(F32)
    expert = jnp.where(lane < slots, pos, -1).astype(F32)
    first = (column(0) == expert).astype(F32)
    second = (column(1) == expert).astype(F32)
    named = first + second
    r_at = lax.broadcasted_iota(jnp.int32, (rows, rows), 0)
    c_at = lax.broadcasted_iota(jnp.int32, (rows, rows), 1)
    earlier = (c_at < r_at).astype(F32).astype(BF16)
    rank = jnp.dot(earlier, named.astype(BF16), preferred_element_type=F32)
    hit = named * (rank == depth).astype(F32)
    w_first, w_second = column(TOP), column(TOP + 1)
    w_sum = w_first + w_second
    mix_w = hit * (first * (w_first / w_sum) + second * (w_second / w_sum))
    pick = hit.T.astype(BF16)[:slots, :]

    loads["gains"].wait()
    loads["resid"].wait()
    gain_rows = gains[...]
    projected = jnp.concatenate([ring_end(k) for k in first_rings], axis=1)
    stream = resid[...].astype(F32) + rms_scale(projected, gain_rows[0:1, :])
    stream_ref[...] = stream
    normed = rms_scale(stream, gain_rows[1:2, :]).astype(BF16)

    outgoing = jnp.dot(pick, normed, preferred_element_type=F32)
    for b in range(folds):
        fold[pl.ds(b, slots, stride=folds), :] = outgoing[
            :, b * LANES : (b + 1) * LANES
        ]
    folded = fold[...].astype(BF16)
    zs[...] = folded
    shift = 3 * n_sp // 16
    my_pos = lax.rem(sp + n_sp - shift, n_sp)
    as_source = pl.ds(pl.multiple_of(my_pos * piece, piece), piece)
    as_expert = pl.ds(pl.multiple_of(sp * piece, piece), piece)
    zr[as_source, :] = zs[as_expert, :]

    with jax.named_scope("above"):

        @pl.when(has_above)
        def _():
            pl.semaphore_wait(all_sem, 1)

    for p in range(1, n_sp):
        d = (p + 1) // 2 if p % 2 else -(p // 2)
        there = lax.rem(sp + d + n_sp, n_sp)
        send(
            zs.at[pl.ds(pl.multiple_of(there * piece, piece), piece), :],
            zr.at[as_source, :],
            z_send.at[0],
            z_recv.at[my_pos],
            {"sp": there},
        )

    came = set()

    def block(cc, other, o):
        return pl.ds(cc * chunk_rows + other * own_rows + (o % chips) * TILE, TILE)

    part_w = width // 2

    def to_partner(cc, part, o):
        c = pl.ds(part * part_w, part_w)
        send(
            xbuf.at[block(cc, 0, o), c],
            xbuf.at[block(cc, 1, o), c],
            gather_send.at[0],
            d_recv.at[cc],
            partner,
        )

    def gather_hop(cc, part, h):
        with jax.named_scope(f"ag{cc}{part}{h}"):
            gather_step(cc, part, h)

    def arrive(src):
        @pl.when(my_pos != src)
        def _():
            settle(zr.at[pl.ds(src * piece, piece), :], z_recv.at[src])

    def gather_step(cc, part, h):
        if h == 1 and part == 0:
            for src in range(n_sp):
                if src not in came and src * piece < (cc + 1) * span:
                    came.add(src)
                    arrive(src)
            fold[pl.ds(cc * span, span), :] = zr[pl.ds(cc * span, span), :].astype(F32)
            for b in range(folds):
                xbuf[block(cc, 0, 0), pl.ds(b * LANES, LANES)] = fold[
                    pl.ds(cc * span + b, TILE, stride=folds), :
                ].astype(BF16)
        elif h > 1:
            settle(
                xbuf.at[pl.ds(0, 2 * TILE), pl.ds(0, part_w)],
                a_recv.at[cc * 2 + part, h - 2],
            )
        for sign, dev, half in ((-1, right, 0), (1, left, 1)):
            c = pl.ds(part * part_w, part_w)
            if h == hops:
                c = pl.ds(part * part_w + half * (part_w // 2), part_w // 2)
            send(
                xbuf.at[block(cc, 0, sign * (h - 1)), c],
                xbuf.at[block(cc, 0, sign * h), c],
                gather_send.at[0],
                a_recv.at[cc * 2 + part, h - 1],
                dev,
            )
        to_partner(cc, part, 1 - h)
        if h > 1:
            to_partner(cc, part, h - 1)

    def gather_last(cc, part):
        with jax.named_scope(f"al{cc}{part}"):
            settle(
                xbuf.at[pl.ds(0, TILE), pl.ds(0, part_w)],
                a_recv.at[cc * 2 + part, hops - 1],
            )
            to_partner(cc, part, hops)

    def experts(cc):
        s = cc + 1
        with jax.named_scope(f"exw{cc}"):
            settle(
                xbuf.at[pl.ds(cc * chunk_rows + own_rows, own_rows), :], d_recv.at[cc]
            )
        with jax.named_scope(f"exc{cc}"):
            x = xbuf[pl.ds(cc * chunk_rows, chunk_rows), :]
            g = jnp.dot(x, wg[...], preferred_element_type=F32)
            u = jnp.dot(x, wu[...], preferred_element_type=F32)
            hid[...] = (g / (1.0 + jnp.exp(-g)) * u).astype(BF16)
            for n in range(width // step_w):
                c = pl.ds(n * step_w, step_w)
                pair_s[s, :, c] = jnp.dot(
                    hid[pl.ds(own_rows, own_rows), :],
                    wd[:, c],
                    preferred_element_type=F32,
                ).astype(BF16)
            for k in set_rings[s]:
                pair_start(k)
            for n in range(width // step_w):
                c = pl.ds(n * step_w, step_w)
                keep[s, :, c] = jnp.dot(
                    hid[pl.ds(0, own_rows), :], wd[:, c], preferred_element_type=F32
                )

    finished = set()
    back_sent = set()
    ended = {}

    def finish(cc, part):
        k = set_rings[cc + 1][part]
        total = ring_end(k)
        first_fold = rings[k][1] // LANES
        for b in range(rings[k][2] // LANES):
            fold[pl.ds(cc * span + first_fold + b, TILE, stride=folds), :] = total[
                :, b * LANES : (b + 1) * LANES
            ]
        ended[cc] = ended.get(cc, 0) + 1
        if ended[cc] < len(set_rings[cc + 1]):
            return
        at = pl.ds(cc * span, span)
        bs[at, :] = fold[at, :].astype(BF16)
        finished.add(cc)
        for p in range(n_sp):
            needs = {p * piece // span, ((p + 1) * piece - 1) // span}
            if p not in back_sent and needs <= finished:
                back_sent.add(p)

                owner = (p + shift) % n_sp

                @pl.when(sp != owner)
                def _():
                    send(
                        bs.at[pl.ds(p * piece, piece), :],
                        br.at[as_expert, :],
                        z_send.at[1],
                        back_recv.at[0],
                        {"sp": owner},
                    )

    for name in ("wg", "wu", "wd"):
        loads[name].wait()
    for op in ORDER:
        if op[0] == 0:
            gather_hop(*op[1:])
        elif op[0] == 4:
            gather_last(*op[1:])
        elif op[0] == 1:
            experts(*op[1:])
        elif op[0] == 2:
            ring_step(set_rings[op[1] + 1][op[2]], op[3])
        else:
            finish(*op[1:])
    br[as_expert, :] = bs[as_source, :]

    far = (n_sp - 1) * piece
    ring_rows = (2 * hops - 1) * TILE
    with jax.named_scope("sendwait"):
        settle(pair_s, pair_send.at[0])
        settle(pair_s.at[:, pl.ds(0, ring_rows), :], ring_send.at[0])
        settle(
            xbuf.at[pl.ds(0, chunks * (ring_rows + own_rows)), :], gather_send.at[0]
        )
        settle(zs.at[pl.ds(piece, far), :], z_send.at[0])

        @pl.when(has_above)
        def _():
            halo.wait_send()

    with jax.named_scope("backwait"):
        settle(br.at[pl.ds(piece, far), :], back_recv.at[0])
    fold[...] = br[...].astype(F32)
    for b in range(folds):
        back[:, pl.ds(b * LANES, LANES)] = fold[
            pl.ds(b, slots, stride=folds), :
        ].astype(BF16)
    mix_w = mix_w[:, :slots]
    mix_hi = mix_w.astype(BF16)
    mix_lo = (mix_w - mix_hi.astype(F32)).astype(BF16)
    picked = back[...]
    combined = jnp.dot(mix_hi, picked, preferred_element_type=F32) + jnp.dot(
        mix_lo, picked, preferred_element_type=F32
    )
    out[...] = stream_ref[...] + rms_scale(combined, gain_rows[2:3, :])
    settle(bs.at[pl.ds(piece, far), :], z_send.at[1])


def per_device(
    resid,
    gate_b,
    gate_c,
    value,
    taps,
    doc_ids,
    out_weight,
    norm_gains,
    routes,
    route_weights,
    w_gate,
    w_up,
    w_down,
):
    n_sp, n_tp = lax.axis_size("sp"), lax.axis_size("tp")
    tok, ch = gate_b.shape
    rows, width = resid.shape
    units = w_gate.shape[2]
    cap = max(2, 3 * TOP * rows // (2 * n_sp))
    chips = n_tp // 2
    hops = chips // 2
    slots = n_sp * cap
    chunks = slots // TILE
    folds = width // LANES
    sets = chunks + 1
    own_rows = chips * TILE
    parts = tok // LANES
    rings = [(0, k * (width // 4), width // 4) for k in range(4)]
    for s in range(1, sets):
        rings += [(s, k * (width // 2), width // 2) for k in range(2)]
    n_rings = len(rings)
    operands = (
        resid,
        gate_b,
        gate_c,
        value,
        taps,
        doc_ids.reshape(parts, LANES),
        out_weight,
        norm_gains,
        routes.T,
        route_weights.T,
        w_gate,
        w_up,
        w_down,
    )
    hbm = pl.BlockSpec(memory_space=pl.ANY)
    vmem = pltpu.VMEM
    dma = pltpu.SemaphoreType.DMA
    result = pl.pallas_call(
        functools.partial(layer_kernel, n_sp, n_tp, cap, rings),
        out_shape=jax.ShapeDtypeStruct((rows, width), F32),
        in_specs=[hbm] * len(operands),
        out_specs=pl.BlockSpec(memory_space=vmem),
        scratch_shapes=[
            *[vmem(a.shape, a.dtype) for a in operands[:10]],
            *[vmem(a.shape[1:], a.dtype) for a in operands[10:]],
            vmem((tok + 8, ch), F32),
            vmem((tok + 8, LANES), F32),
            vmem((16, ch), F32),
            vmem((16, ch), F32),
            vmem((tok, ch), BF16),
            vmem((2, own_rows, ch), BF16),
            vmem((2 * TOP * parts, LANES), F32),
            vmem((LANES, LANES), F32),
            vmem((slots * folds, LANES), BF16),
            vmem((slots * folds, LANES), BF16),
            vmem((slots * folds, LANES), BF16),
            vmem((slots * folds, LANES), BF16),
            vmem((slots * folds, LANES), F32),
            vmem((chunks * n_tp * TILE, width), BF16),
            vmem((n_tp * TILE, units), BF16),
            vmem((sets, own_rows, width), BF16),
            vmem((sets, own_rows, width), BF16),
            vmem((sets, own_rows, width), F32),
            vmem((sets, chips, TILE, width), BF16),
            vmem((sets, hops, TILE, width), BF16),
            vmem((sets, hops, TILE, width), BF16),
            vmem((rows, width), F32),
            vmem((slots, width), BF16),
            dma((len(operands),)),
            dma((2,)),
            pltpu.SemaphoreType.REGULAR,
            pltpu.SemaphoreType.REGULAR,
            dma((2,)),
            dma((n_sp,)),
            dma((1,)),
            dma((1,)),
            dma((n_rings,)),
            dma((1,)),
            dma((n_rings, hops)),
            dma((1,)),
            dma((chunks,)),
            dma((chunks * 2, hops)),
        ],
        compiler_params=pltpu.CompilerParams(
            collective_id=0,
            has_side_effects=True,
            vmem_limit_bytes=56 * 1024 * 1024,
        ),
        name="layer",
    )(*operands)
    return result.astype(BF16)


def solution(mesh):
    return jax.shard_map(
        per_device,
        mesh=mesh,
        in_specs=(
            P(("grp", "sp", "tp"), None),
            P(("grp", "sp"), "tp"),
            P(("grp", "sp"), "tp"),
            P(("grp", "sp"), "tp"),
            P(None, "tp"),
            P(("grp", "sp")),
            P("tp", None),
            P(),
            P(("grp", "sp"), None),
            P(("grp", "sp"), None),
            P("sp", None, "tp"),
            P("sp", None, "tp"),
            P("sp", "tp", None),
        ),
        out_specs=P(("grp", "sp", "tp"), None),
        check_vma=False,
    )
```

```python
import functools

import jax
import jax.numpy as jnp
from jax import lax
from jax.experimental import pallas as pl
from jax.experimental.pallas import tpu as pltpu
from jax.sharding import PartitionSpec as P

TAPS = 3
TOP = 2
LANES = 128
TILE = 16

norm_eps = 1e-06

ORDER = (
    (0, 0, 0, 1), (0, 0, 1, 1), (0, 1, 0, 1), (0, 1, 1, 1), (0, 0, 0, 2),
    (0, 0, 1, 2), (0, 1, 0, 2), (0, 1, 1, 2), (0, 2, 0, 1), (0, 2, 1, 1),
    (0, 0, 0, 3), (0, 0, 1, 3), (0, 1, 0, 3), (0, 1, 1, 3), (0, 2, 0, 2),
    (0, 2, 1, 2), (0, 0, 0, 4), (0, 0, 1, 4), (0, 1, 0, 4), (0, 1, 1, 4),
    (0, 2, 0, 3), (0, 2, 1, 3), (4, 0, 0), (4, 0, 1), (4, 1, 0),
    (1, 0), (4, 1, 1), (0, 2, 0, 4), (0, 2, 1, 4), (1, 1),
    (2, 0, 0, 1), (2, 0, 1, 1), (4, 2, 0), (4, 2, 1), (2, 1, 0, 1),
    (2, 1, 1, 1), (1, 2), (2, 0, 0, 2), (2, 0, 1, 2), (2, 2, 0, 1),
    (2, 2, 1, 1), (2, 1, 0, 2), (2, 1, 1, 2), (2, 0, 0, 3), (2, 2, 0, 2),
    (2, 2, 1, 2), (2, 0, 1, 3), (2, 1, 0, 3), (2, 1, 1, 3), (2, 0, 0, 4),
    (2, 2, 0, 3), (2, 2, 1, 3), (2, 0, 1, 4), (2, 1, 0, 4), (2, 1, 1, 4),
    (3, 0, 0), (2, 2, 0, 4), (2, 2, 1, 4), (3, 0, 1), (3, 1, 0),
    (3, 1, 1), (3, 2, 0), (3, 2, 1),
)
BF16 = jnp.bfloat16
F32 = jnp.float32
MESH = pl.DeviceIdType.MESH


def rms_scale(values, gain_row):
    mean_sq = jnp.mean(values * values, axis=-1, keepdims=True)
    return values * lax.rsqrt(mean_sq + norm_eps) * gain_row


def layer_kernel(
    n_sp,
    n_tp,
    cap,
    rings,
    resid_h,
    gate_b_h,
    gate_c_h,
    value_h,
    taps_h,
    ids_h,
    out_w_h,
    gains_h,
    routes_h,
    route_w_h,
    w_gate_h,
    w_up_h,
    w_down_h,
    out,
    resid,
    gate_b,
    gate_c,
    value,
    taps,
    ids,
    ow,
    gains,
    routes,
    route_w,
    wg,
    wu,
    wd,
    ext,
    ext_ids,
    halo_s,
    halo_r,
    mixed,
    sel,
    table,
    columns,
    zs,
    zr,
    bs,
    br,
    fold,
    xbuf,
    hid,
    pair_s,
    pair_r,
    keep,
    ring_s,
    ring_r,
    ring_l,
    stream_ref,
    back,
    load_sem,
    halo_sem,
    below_sem,
    all_sem,
    z_send,
    z_recv,
    back_recv,
    pair_send,
    pair_recv,
    ring_send,
    r_recv,
    gather_send,
    d_recv,
    a_recv,
):
    tok, ch = gate_b.shape
    rows, width = resid.shape
    chips = n_tp // 2
    hops = chips // 2
    folds = width // LANES
    slots = n_sp * cap
    chunks = slots // TILE
    chunk_rows = n_tp * TILE
    own_rows = chips * TILE
    piece = cap * folds
    span = TILE * folds

    tp = lax.axis_index("tp")
    sp = lax.axis_index("sp")
    core = lax.rem(tp, 2)
    chip = lax.div(tp, 2)
    partner = {"tp": chip * 2 + (1 - core)}
    right = {"tp": lax.rem(chip + 1, chips) * 2 + core}
    left = {"tp": lax.rem(chip + chips - 1, chips) * 2 + core}

    def along(d):
        return {"sp": lax.rem(sp + d + n_sp, n_sp)}

    def remote(src, dst, s_sem, r_sem, dev):
        return pltpu.make_async_remote_copy(
            src_ref=src,
            dst_ref=dst,
            send_sem=s_sem,
            recv_sem=r_sem,
            device_id=dev,
            device_id_type=MESH,
        )

    def send(src, dst, s_sem, r_sem, dev):
        copy = remote(src, dst, s_sem, r_sem, dev)
        copy.start()
        return copy

    def settle(ref, sem):
        pltpu.make_async_copy(ref, ref, sem).wait()

    barrier = pltpu.get_barrier_semaphore()
    greeted = [partner, right, left, along(-1), along(1)]
    for dev in greeted:
        pl.semaphore_signal(barrier, inc=1, device_id=dev, device_id_type=MESH)
    last = n_sp - 1
    has_below, has_above = sp > 0, sp < last

    loads = {}
    for i, (name, src, dst) in enumerate(
        (
            ("ids", ids_h, ids),
            ("gate_c", gate_c_h, gate_c),
            ("value", value_h, value),
            ("gate_b", gate_b_h, gate_b),
            ("taps", taps_h, taps),
            ("ow", out_w_h, ow),
            ("routes", routes_h, routes),
            ("route_w", route_w_h, route_w),
            ("gains", gains_h, gains),
            ("resid", resid_h, resid),
            ("wg", w_gate_h.at[0], wg),
            ("wu", w_up_h.at[0], wu),
            ("wd", w_down_h.at[0], wd),
        )
    ):
        loads[name] = pltpu.make_async_copy(src, dst, load_sem.at[i])
        loads[name].start()

    parts = tok // LANES
    loads["ids"].wait()
    for k in range(parts):
        line = ids[k : k + 1, :].astype(F32)
        ext_ids[pl.ds(8 + k * LANES, LANES), :] = jnp.broadcast_to(
            line, (LANES, LANES)
        ).T
    loads["gate_c"].wait()
    loads["value"].wait()
    product = gate_c[...].astype(F32) * value[...].astype(F32)
    ext[pl.ds(8, tok), :] = product
    halo_s[pl.ds(0, 8), :] = product[tok - 8 :]
    halo_s[pl.ds(8, 8), :] = ext_ids[pl.ds(tok, 8), :]

    with jax.named_scope("barrier"):
        pl.semaphore_wait(barrier, len(greeted))
    halo = remote(halo_s, halo_r, halo_sem.at[0], halo_sem.at[1], along(1))

    @pl.when(has_above)
    def _():
        halo.start()

    with jax.named_scope("chain"):

        @pl.when(sp > 2)
        def _():
            pl.semaphore_wait(below_sem, 1)

        @pl.when((sp >= 2) & has_above)
        def _():
            pl.semaphore_signal(
                below_sem, inc=1, device_id=along(1), device_id_type=MESH
            )

        @pl.when(sp == 0)
        def _():
            pl.semaphore_signal(
                all_sem, inc=1, device_id=along(-1), device_id_type=MESH
            )

    ext[pl.ds(0, 8), :] = jnp.zeros((8, ch), F32)
    ext_ids[pl.ds(0, 8), :] = jnp.full((8, LANES), -1.0, F32)
    loads["gate_b"].wait()
    loads["taps"].wait()

    @pl.when(has_below)
    def _():
        halo.wait_recv()
        ext[pl.ds(0, 8), :] = halo_r[pl.ds(0, 8), :]
        ext_ids[pl.ds(0, 8), :] = halo_r[pl.ds(8, 8), :]

    here = ext_ids[pl.ds(8, tok), :]
    tap_rows = taps[...].astype(F32)
    conv = tap_rows[0:1, :] * ext[pl.ds(8, tok), :]
    for lag in range(1, TAPS):
        same = ext_ids[pl.ds(8 - lag, tok), :] == here
        conv = conv + jnp.where(
            same, tap_rows[lag : lag + 1, :] * ext[pl.ds(8 - lag, tok), :], 0.0
        )
    mixed[...] = (gate_b[...].astype(F32) * conv).astype(BF16)

    def place(owner, o):
        block = lax.rem(chip + o, chips) * 2 + owner
        return pl.ds(pl.multiple_of(block * rows, rows), rows)

    for o in range(chips):
        sel[0, pl.ds(o * rows, rows), :] = mixed[place(core, o), :]
        sel[1, pl.ds(o * rows, rows), :] = mixed[place(1 - core, o), :]

    ring = {}

    def pair_start(k):
        s, at, cols = rings[k]
        at = pl.ds(at, cols)
        ring[k, "pair"] = send(
            pair_s.at[s, :, at],
            pair_r.at[s, :, at],
            pair_send.at[0],
            pair_recv.at[k],
            partner,
        )

    def hop_wait(k, h):
        _, at, cols = rings[k]
        settle(
            pair_r.at[0, pl.ds(0, TILE if h == 1 else 2 * TILE), pl.ds(at, cols)],
            r_recv.at[k, h - 1],
        )

    def ring_step(k, h):
        with jax.named_scope(f"rs{k}_{h}"):
            ring_hop(k, h)

    def ring_hop(k, h):
        s, at, cols = rings[k]
        all_c = pl.ds(at, cols)
        lo, hi = pl.ds(at, cols // 2), pl.ds(at + cols // 2, cols // 2)

        def share(o, c):
            r = pl.ds(o * TILE, TILE)
            return keep[s, r, c] + pair_r[s, r, c].astype(F32)

        if h == 1:
            ring[k, "pair"].wait_recv()
            ring_s[s, hops, :, all_c] = share(hops, all_c).astype(BF16)
        else:
            hop_wait(k, h - 1)
        for buf, dev, early, late, o in (
            (ring_r, right, lo, hi, hops + 1 - h),
            (ring_l, left, hi, lo, (chips - hops - 1 + h) % chips),
        ):
            if h == 2:
                ring_s[s, o, :, early] = (
                    share(o, early) + buf[s, 0, :, early].astype(F32)
                ).astype(BF16)
                ring_s[s, o, :, late] = share(o, late).astype(BF16)
            elif h > 2:
                ring_s[s, o, :, all_c] = (
                    share(o, all_c) + buf[s, h - 2, :, all_c].astype(F32)
                ).astype(BF16)
            c = early if h == 1 else all_c
            send(
                ring_s.at[s, o, :, c],
                buf.at[s, h - 1, :, c],
                ring_send.at[0],
                r_recv.at[k, h - 1],
                dev,
            )

    def ring_end(k):
        with jax.named_scope(f"re{k}"):
            s, at, cols = rings[k]
            c = pl.ds(at, cols)
            hop_wait(k, hops)
            return (
                keep[s, pl.ds(0, TILE), c]
                + pair_r[s, pl.ds(0, TILE), c].astype(F32)
                + ring_r[s, hops - 1, :, c].astype(F32)
                + ring_l[s, hops - 1, :, c].astype(F32)
            )

    set_rings = {}
    for k, (s, _, _) in enumerate(rings):
        set_rings.setdefault(s, []).append(k)
    first_rings = set_rings[0]
    loads["ow"].wait()
    step_w = min(512, width)
    for k in first_rings:
        _, at, cols = rings[k]
        for n in range(cols // step_w):
            c = pl.ds(at + n * step_w, step_w)
            pair_s[0, :, c] = jnp.dot(
                sel[1], ow[:, c], preferred_element_type=F32
            ).astype(BF16)
        pair_start(k)
    @pl.when(sp == last)
    def _():
        pl.semaphore_wait(all_sem, 1)
        for there in range(last):
            pl.semaphore_signal(
                all_sem, inc=1, device_id={"sp": there}, device_id_type=MESH
            )

    for n in range(width // step_w):
        c = pl.ds(n * step_w, step_w)
        keep[0, :, c] = jnp.dot(sel[0], ow[:, c], preferred_element_type=F32)
    for h in range(1, hops + 1):
        for k in first_rings:
            ring_step(k, h)

    loads["routes"].wait()
    loads["route_w"].wait()
    for k in range(TOP):
        for part in range(parts):
            c = pl.ds(part * LANES, LANES)
            table[pl.ds(k * parts + part, 1), :] = routes[pl.ds(k, 1), c].astype(F32)
            table[pl.ds((TOP + k) * parts + part, 1), :] = route_w[pl.ds(k, 1), c]
    columns[:, pl.ds(0, 2 * TOP * parts)] = table[...].T
    base = tp * rows
    my_part = lax.div(base, LANES)
    mine = columns[pl.ds(pl.multiple_of(base - my_part * LANES, rows), rows), :]

    def column(n):
        found = mine[:, n * parts : n * parts + 1]
        for part in range(1, parts):
            found = jnp.where(
                my_part == part, mine[:, n * parts + part : n * parts + part + 1], found
            )
        return found

    lane = lax.broadcasted_iota(jnp.int32, (rows, LANES), 1)
    pos = jnp.floor((lane.astype(F32) + 0.5) * (1.0 / cap)).astype(jnp.int32)
    depth = (lane - pos * cap).astype(F32)
    expert = jnp.where(lane < slots, pos, -1).astype(F32)
    first = (column(0) == expert).astype(F32)
    second = (column(1) == expert).astype(F32)
    named = first + second
    r_at = lax.broadcasted_iota(jnp.int32, (rows, rows), 0)
    c_at = lax.broadcasted_iota(jnp.int32, (rows, rows), 1)
    earlier = (c_at < r_at).astype(F32).astype(BF16)
    rank = jnp.dot(earlier, named.astype(BF16), preferred_element_type=F32)
    hit = named * (rank == depth).astype(F32)
    w_first, w_second = column(TOP), column(TOP + 1)
    w_sum = w_first + w_second
    mix_w = hit * (first * (w_first / w_sum) + second * (w_second / w_sum))
    pick = hit.T.astype(BF16)[:slots, :]

    loads["gains"].wait()
    loads["resid"].wait()
    gain_rows = gains[...]
    projected = jnp.concatenate([ring_end(k) for k in first_rings], axis=1)
    stream = resid[...].astype(F32) + rms_scale(projected, gain_rows[0:1, :])
    stream_ref[...] = stream
    normed = rms_scale(stream, gain_rows[1:2, :]).astype(BF16)

    outgoing = jnp.dot(pick, normed, preferred_element_type=F32)
    for b in range(folds):
        fold[pl.ds(b, slots, stride=folds), :] = outgoing[
            :, b * LANES : (b + 1) * LANES
        ]
    folded = fold[...].astype(BF16)
    zs[...] = folded
    shift = 3 * n_sp // 16
    my_pos = lax.rem(sp + n_sp - shift, n_sp)
    as_source = pl.ds(pl.multiple_of(my_pos * piece, piece), piece)
    as_expert = pl.ds(pl.multiple_of(sp * piece, piece), piece)
    zr[as_source, :] = zs[as_expert, :]

    with jax.named_scope("above"):

        @pl.when(has_above)
        def _():
            pl.semaphore_wait(all_sem, 1)

    for p in reversed(range(1, n_sp)):
        d = (p + 1) // 2 if p % 2 else -(p // 2)
        there = lax.rem(sp + d + n_sp, n_sp)
        send(
            zs.at[pl.ds(pl.multiple_of(there * piece, piece), piece), :],
            zr.at[as_source, :],
            z_send.at[0],
            z_recv.at[my_pos],
            {"sp": there},
        )

    came = set()

    def block(cc, other, o):
        return pl.ds(cc * chunk_rows + other * own_rows + (o % chips) * TILE, TILE)

    part_w = width // 2

    def to_partner(cc, part, o):
        c = pl.ds(part * part_w, part_w)
        send(
            xbuf.at[block(cc, 0, o), c],
            xbuf.at[block(cc, 1, o), c],
            gather_send.at[0],
            d_recv.at[cc],
            partner,
        )

    def gather_hop(cc, part, h):
        with jax.named_scope(f"ag{cc}{part}{h}"):
            gather_step(cc, part, h)

    def arrive(src):
        @pl.when(my_pos != src)
        def _():
            settle(zr.at[pl.ds(src * piece, piece), :], z_recv.at[src])

    def gather_step(cc, part, h):
        if h == 1 and part == 0:
            for src in range(n_sp):
                if src not in came and src * piece < (cc + 1) * span:
                    came.add(src)
                    arrive(src)
            fold[pl.ds(cc * span, span), :] = zr[pl.ds(cc * span, span), :].astype(F32)
            for b in range(folds):
                xbuf[block(cc, 0, 0), pl.ds(b * LANES, LANES)] = fold[
                    pl.ds(cc * span + b, TILE, stride=folds), :
                ].astype(BF16)
        elif h > 1:
            settle(
                xbuf.at[pl.ds(0, 2 * TILE), pl.ds(0, part_w)],
                a_recv.at[cc * 2 + part, h - 2],
            )
        for sign, dev, half in ((-1, right, 0), (1, left, 1)):
            c = pl.ds(part * part_w, part_w)
            if h == hops:
                c = pl.ds(part * part_w + half * (part_w // 2), part_w // 2)
            send(
                xbuf.at[block(cc, 0, sign * (h - 1)), c],
                xbuf.at[block(cc, 0, sign * h), c],
                gather_send.at[0],
                a_recv.at[cc * 2 + part, h - 1],
                dev,
            )
        to_partner(cc, part, 1 - h)
        if h > 1:
            to_partner(cc, part, h - 1)

    def gather_last(cc, part):
        with jax.named_scope(f"al{cc}{part}"):
            settle(
                xbuf.at[pl.ds(0, TILE), pl.ds(0, part_w)],
                a_recv.at[cc * 2 + part, hops - 1],
            )
            to_partner(cc, part, hops)

    def experts(cc):
        s = cc + 1
        with jax.named_scope(f"exw{cc}"):
            settle(
                xbuf.at[pl.ds(cc * chunk_rows + own_rows, own_rows), :], d_recv.at[cc]
            )
        with jax.named_scope(f"exc{cc}"):
            x = xbuf[pl.ds(cc * chunk_rows, chunk_rows), :]
            g = jnp.dot(x, wg[...], preferred_element_type=F32)
            u = jnp.dot(x, wu[...], preferred_element_type=F32)
            hid[...] = (g / (1.0 + jnp.exp(-g)) * u).astype(BF16)
            for k in set_rings[s]:
                _, at, cols = rings[k]
                for n in range(cols // step_w):
                    c = pl.ds(at + n * step_w, step_w)
                    pair_s[s, :, c] = jnp.dot(
                        hid[pl.ds(own_rows, own_rows), :],
                        wd[:, c],
                        preferred_element_type=F32,
                    ).astype(BF16)
                pair_start(k)
            for n in range(width // step_w):
                c = pl.ds(n * step_w, step_w)
                keep[s, :, c] = jnp.dot(
                    hid[pl.ds(0, own_rows), :], wd[:, c], preferred_element_type=F32
                )

    finished = set()
    back_sent = set()
    ended = {}

    def finish(cc, part):
        k = set_rings[cc + 1][part]
        total = ring_end(k)
        first_fold = rings[k][1] // LANES
        for b in range(rings[k][2] // LANES):
            fold[pl.ds(cc * span + first_fold + b, TILE, stride=folds), :] = total[
                :, b * LANES : (b + 1) * LANES
            ]
        ended[cc] = ended.get(cc, 0) + 1
        if ended[cc] < len(set_rings[cc + 1]):
            return
        at = pl.ds(cc * span, span)
        bs[at, :] = fold[at, :].astype(BF16)
        finished.add(cc)
        for p in range(n_sp):
            needs = {p * piece // span, ((p + 1) * piece - 1) // span}
            if p not in back_sent and needs <= finished:
                back_sent.add(p)

                owner = (p + shift) % n_sp

                @pl.when(sp != owner)
                def _():
                    send(
                        bs.at[pl.ds(p * piece, piece), :],
                        br.at[as_expert, :],
                        z_send.at[1],
                        back_recv.at[0],
                        {"sp": owner},
                    )

    for name in ("wg", "wu", "wd"):
        loads[name].wait()
    for op in ORDER:
        if op[0] == 0:
            gather_hop(*op[1:])
        elif op[0] == 4:
            gather_last(*op[1:])
        elif op[0] == 1:
            experts(*op[1:])
        elif op[0] == 2:
            ring_step(set_rings[op[1] + 1][op[2]], op[3])
        else:
            finish(*op[1:])
    br[as_expert, :] = bs[as_source, :]

    far = (n_sp - 1) * piece
    ring_rows = (2 * hops - 1) * TILE
    with jax.named_scope("sendwait"):
        settle(pair_s, pair_send.at[0])
        settle(pair_s.at[:, pl.ds(0, ring_rows), :], ring_send.at[0])
        settle(
            xbuf.at[pl.ds(0, chunks * (ring_rows + own_rows)), :], gather_send.at[0]
        )
        settle(zs.at[pl.ds(piece, far), :], z_send.at[0])

        @pl.when(has_above)
        def _():
            halo.wait_send()

    with jax.named_scope("backwait"):
        settle(br.at[pl.ds(piece, far), :], back_recv.at[0])
    fold[...] = br[...].astype(F32)
    for b in range(folds):
        back[:, pl.ds(b * LANES, LANES)] = fold[
            pl.ds(b, slots, stride=folds), :
        ].astype(BF16)
    mix_w = mix_w[:, :slots]
    mix_hi = mix_w.astype(BF16)
    mix_lo = (mix_w - mix_hi.astype(F32)).astype(BF16)
    picked = back[...]
    combined = jnp.dot(mix_hi, picked, preferred_element_type=F32) + jnp.dot(
        mix_lo, picked, preferred_element_type=F32
    )
    out[...] = stream_ref[...] + rms_scale(combined, gain_rows[2:3, :])
    settle(bs.at[pl.ds(piece, far), :], z_send.at[1])


def per_device(
    resid,
    gate_b,
    gate_c,
    value,
    taps,
    doc_ids,
    out_weight,
    norm_gains,
    routes,
    route_weights,
    w_gate,
    w_up,
    w_down,
):
    n_sp, n_tp = lax.axis_size("sp"), lax.axis_size("tp")
    tok, ch = gate_b.shape
    rows, width = resid.shape
    units = w_gate.shape[2]
    cap = max(2, 3 * TOP * rows // (2 * n_sp))
    chips = n_tp // 2
    hops = chips // 2
    slots = n_sp * cap
    chunks = slots // TILE
    folds = width // LANES
    sets = chunks + 1
    own_rows = chips * TILE
    parts = tok // LANES
    rings = [(0, k * (width // 4), width // 4) for k in range(4)]
    for s in range(1, sets):
        rings += [(s, k * (width // 2), width // 2) for k in range(2)]
    n_rings = len(rings)
    operands = (
        resid,
        gate_b,
        gate_c,
        value,
        taps,
        doc_ids.reshape(parts, LANES),
        out_weight,
        norm_gains,
        routes.T,
        route_weights.T,
        w_gate,
        w_up,
        w_down,
    )
    hbm = pl.BlockSpec(memory_space=pl.ANY)
    vmem = pltpu.VMEM
    dma = pltpu.SemaphoreType.DMA
    result = pl.pallas_call(
        functools.partial(layer_kernel, n_sp, n_tp, cap, rings),
        out_shape=jax.ShapeDtypeStruct((rows, width), F32),
        in_specs=[hbm] * len(operands),
        out_specs=pl.BlockSpec(memory_space=vmem),
        scratch_shapes=[
            *[vmem(a.shape, a.dtype) for a in operands[:10]],
            *[vmem(a.shape[1:], a.dtype) for a in operands[10:]],
            vmem((tok + 8, ch), F32),
            vmem((tok + 8, LANES), F32),
            vmem((16, ch), F32),
            vmem((16, ch), F32),
            vmem((tok, ch), BF16),
            vmem((2, own_rows, ch), BF16),
            vmem((2 * TOP * parts, LANES), F32),
            vmem((LANES, LANES), F32),
            vmem((slots * folds, LANES), BF16),
            vmem((slots * folds, LANES), BF16),
            vmem((slots * folds, LANES), BF16),
            vmem((slots * folds, LANES), BF16),
            vmem((slots * folds, LANES), F32),
            vmem((chunks * n_tp * TILE, width), BF16),
            vmem((n_tp * TILE, units), BF16),
            vmem((sets, own_rows, width), BF16),
            vmem((sets, own_rows, width), BF16),
            vmem((sets, own_rows, width), F32),
            vmem((sets, chips, TILE, width), BF16),
            vmem((sets, hops, TILE, width), BF16),
            vmem((sets, hops, TILE, width), BF16),
            vmem((rows, width), F32),
            vmem((slots, width), BF16),
            dma((len(operands),)),
            dma((2,)),
            pltpu.SemaphoreType.REGULAR,
            pltpu.SemaphoreType.REGULAR,
            dma((2,)),
            dma((n_sp,)),
            dma((1,)),
            dma((1,)),
            dma((n_rings,)),
            dma((1,)),
            dma((n_rings, hops)),
            dma((1,)),
            dma((chunks,)),
            dma((chunks * 2, hops)),
        ],
        compiler_params=pltpu.CompilerParams(
            collective_id=0,
            has_side_effects=True,
            vmem_limit_bytes=56 * 1024 * 1024,
        ),
        name="layer",
    )(*operands)
    return result.astype(BF16)


def solution(mesh):
    return jax.shard_map(
        per_device,
        mesh=mesh,
        in_specs=(
            P(("grp", "sp", "tp"), None),
            P(("grp", "sp"), "tp"),
            P(("grp", "sp"), "tp"),
            P(("grp", "sp"), "tp"),
            P(None, "tp"),
            P(("grp", "sp")),
            P("tp", None),
            P(),
            P(("grp", "sp"), None),
            P(("grp", "sp"), None),
            P("sp", None, "tp"),
            P("sp", None, "tp"),
            P("sp", "tp", None),
        ),
        out_specs=P(("grp", "sp", "tp"), None),
        check_vma=False,
    )
```

```python
import functools

import jax
import jax.numpy as jnp
from jax import lax
from jax.experimental import pallas as pl
from jax.experimental.pallas import tpu as pltpu
from jax.sharding import PartitionSpec as P

TAPS = 3
TOP = 2
LANES = 128
TILE = 16

norm_eps = 1e-06

ORDER = (
    (0, 0, 0, 1), (0, 0, 1, 1), (0, 1, 0, 1), (0, 1, 1, 1), (0, 0, 0, 2),
    (0, 0, 1, 2), (0, 1, 0, 2), (0, 1, 1, 2), (0, 2, 0, 1), (0, 2, 1, 1),
    (0, 0, 0, 3), (0, 0, 1, 3), (0, 1, 0, 3), (0, 1, 1, 3), (0, 2, 0, 2),
    (0, 2, 1, 2), (0, 0, 0, 4), (0, 0, 1, 4), (0, 1, 0, 4), (0, 1, 1, 4),
    (0, 2, 0, 3), (0, 2, 1, 3), (4, 0, 0), (4, 0, 1), (4, 1, 0),
    (1, 0), (4, 1, 1), (0, 2, 0, 4), (0, 2, 1, 4), (2, 0, 0, 1),
    (2, 0, 1, 1), (1, 1), (4, 2, 0), (4, 2, 1), (2, 1, 0, 1),
    (2, 1, 1, 1), (1, 2), (2, 0, 0, 2), (2, 0, 1, 2), (2, 2, 0, 1),
    (2, 2, 1, 1), (2, 1, 0, 2), (2, 1, 1, 2), (2, 0, 0, 3), (2, 0, 1, 3),
    (2, 2, 0, 2), (2, 2, 1, 2), (2, 1, 0, 3), (2, 1, 1, 3), (2, 0, 0, 4),
    (2, 0, 1, 4), (2, 2, 0, 3), (2, 2, 1, 3), (2, 1, 0, 4), (2, 1, 1, 4),
    (3, 0, 0), (3, 0, 1), (2, 2, 0, 4), (2, 2, 1, 4), (3, 1, 0),
    (3, 1, 1), (3, 2, 0), (3, 2, 1),
)
BF16 = jnp.bfloat16
F32 = jnp.float32
MESH = pl.DeviceIdType.MESH


def rms_scale(values, gain_row):
    mean_sq = jnp.mean(values * values, axis=-1, keepdims=True)
    return values * lax.rsqrt(mean_sq + norm_eps) * gain_row


def layer_kernel(
    n_sp,
    n_tp,
    cap,
    rings,
    resid_h,
    gate_b_h,
    gate_c_h,
    value_h,
    taps_h,
    ids_h,
    out_w_h,
    gains_h,
    routes_h,
    route_w_h,
    w_gate_h,
    w_up_h,
    w_down_h,
    out,
    resid,
    gate_b,
    gate_c,
    value,
    taps,
    ids,
    ow,
    gains,
    routes,
    route_w,
    wg,
    wu,
    wd,
    ext,
    ext_ids,
    halo_s,
    halo_r,
    mixed,
    sel,
    table,
    columns,
    zs,
    zr,
    bs,
    br,
    fold,
    xbuf,
    hid,
    pair_s,
    pair_r,
    keep,
    ring_s,
    ring_r,
    ring_l,
    stream_ref,
    back,
    load_sem,
    halo_sem,
    below_sem,
    all_sem,
    z_send,
    z_recv,
    back_recv,
    pair_send,
    pair_recv,
    ring_send,
    r_recv,
    gather_send,
    d_recv,
    a_recv,
):
    tok, ch = gate_b.shape
    rows, width = resid.shape
    chips = n_tp // 2
    hops = chips // 2
    folds = width // LANES
    slots = n_sp * cap
    chunks = slots // TILE
    chunk_rows = n_tp * TILE
    own_rows = chips * TILE
    piece = cap * folds
    span = TILE * folds

    tp = lax.axis_index("tp")
    sp = lax.axis_index("sp")
    core = lax.rem(tp, 2)
    chip = lax.div(tp, 2)
    partner = {"tp": chip * 2 + (1 - core)}
    right = {"tp": lax.rem(chip + 1, chips) * 2 + core}
    left = {"tp": lax.rem(chip + chips - 1, chips) * 2 + core}

    def along(d):
        return {"sp": lax.rem(sp + d + n_sp, n_sp)}

    def remote(src, dst, s_sem, r_sem, dev):
        return pltpu.make_async_remote_copy(
            src_ref=src,
            dst_ref=dst,
            send_sem=s_sem,
            recv_sem=r_sem,
            device_id=dev,
            device_id_type=MESH,
        )

    def send(src, dst, s_sem, r_sem, dev):
        copy = remote(src, dst, s_sem, r_sem, dev)
        copy.start()
        return copy

    def settle(ref, sem):
        pltpu.make_async_copy(ref, ref, sem).wait()

    barrier = pltpu.get_barrier_semaphore()
    greeted = [partner, right, left, along(-1), along(1)]
    for dev in greeted:
        pl.semaphore_signal(barrier, inc=1, device_id=dev, device_id_type=MESH)
    last = n_sp - 1
    has_below, has_above = sp > 0, sp < last

    loads = {}
    for i, (name, src, dst) in enumerate(
        (
            ("ids", ids_h, ids),
            ("gate_c", gate_c_h, gate_c),
            ("value", value_h, value),
            ("gate_b", gate_b_h, gate_b),
            ("taps", taps_h, taps),
            ("ow", out_w_h, ow),
            ("routes", routes_h, routes),
            ("route_w", route_w_h, route_w),
            ("gains", gains_h, gains),
            ("resid", resid_h, resid),
            ("wg", w_gate_h.at[0], wg),
            ("wu", w_up_h.at[0], wu),
            ("wd", w_down_h.at[0], wd),
        )
    ):
        loads[name] = pltpu.make_async_copy(src, dst, load_sem.at[i])
        loads[name].start()

    parts = tok // LANES
    loads["ids"].wait()
    for k in range(parts):
        line = ids[k : k + 1, :].astype(F32)
        ext_ids[pl.ds(8 + k * LANES, LANES), :] = jnp.broadcast_to(
            line, (LANES, LANES)
        ).T
    loads["gate_c"].wait()
    loads["value"].wait()
    product = gate_c[...].astype(F32) * value[...].astype(F32)
    ext[pl.ds(8, tok), :] = product
    halo_s[pl.ds(0, 8), :] = product[tok - 8 :]
    halo_s[pl.ds(8, 8), :] = ext_ids[pl.ds(tok, 8), :]

    with jax.named_scope("barrier"):
        pl.semaphore_wait(barrier, len(greeted))
    halo = remote(halo_s, halo_r, halo_sem.at[0], halo_sem.at[1], along(1))

    @pl.when(has_above)
    def _():
        halo.start()

    with jax.named_scope("chain"):

        @pl.when(sp > 2)
        def _():
            pl.semaphore_wait(below_sem, 1)

        @pl.when((sp >= 2) & has_above)
        def _():
            pl.semaphore_signal(
                below_sem, inc=1, device_id=along(1), device_id_type=MESH
            )

        @pl.when(sp == 0)
        def _():
            pl.semaphore_signal(
                all_sem, inc=1, device_id=along(-1), device_id_type=MESH
            )

    ext[pl.ds(0, 8), :] = jnp.zeros((8, ch), F32)
    ext_ids[pl.ds(0, 8), :] = jnp.full((8, LANES), -1.0, F32)
    loads["gate_b"].wait()
    loads["taps"].wait()

    @pl.when(has_below)
    def _():
        halo.wait_recv()
        ext[pl.ds(0, 8), :] = halo_r[pl.ds(0, 8), :]
        ext_ids[pl.ds(0, 8), :] = halo_r[pl.ds(8, 8), :]

    here = ext_ids[pl.ds(8, tok), :]
    tap_rows = taps[...].astype(F32)
    conv = tap_rows[0:1, :] * ext[pl.ds(8, tok), :]
    for lag in range(1, TAPS):
        same = ext_ids[pl.ds(8 - lag, tok), :] == here
        conv = conv + jnp.where(
            same, tap_rows[lag : lag + 1, :] * ext[pl.ds(8 - lag, tok), :], 0.0
        )
    mixed[...] = (gate_b[...].astype(F32) * conv).astype(BF16)

    def place(owner, o):
        block = lax.rem(chip + o, chips) * 2 + owner
        return pl.ds(pl.multiple_of(block * rows, rows), rows)

    for o in range(chips):
        sel[0, pl.ds(o * rows, rows), :] = mixed[place(core, o), :]
        sel[1, pl.ds(o * rows, rows), :] = mixed[place(1 - core, o), :]

    ring = {}

    def pair_start(k):
        s, at, cols = rings[k]
        at = pl.ds(at, cols)
        ring[k, "pair"] = send(
            pair_s.at[s, :, at],
            pair_r.at[s, :, at],
            pair_send.at[0],
            pair_recv.at[k],
            partner,
        )

    def hop_wait(k, h):
        _, at, cols = rings[k]
        settle(
            pair_r.at[0, pl.ds(0, TILE if h == 1 else 2 * TILE), pl.ds(at, cols)],
            r_recv.at[k, h - 1],
        )

    def ring_step(k, h):
        with jax.named_scope(f"rs{k}_{h}"):
            ring_hop(k, h)

    def ring_hop(k, h):
        s, at, cols = rings[k]
        all_c = pl.ds(at, cols)
        lo, hi = pl.ds(at, cols // 2), pl.ds(at + cols // 2, cols // 2)

        def share(o, c):
            r = pl.ds(o * TILE, TILE)
            return keep[s, r, c] + pair_r[s, r, c].astype(F32)

        if h == 1:
            ring[k, "pair"].wait_recv()
            ring_s[s, hops, :, all_c] = share(hops, all_c).astype(BF16)
        else:
            hop_wait(k, h - 1)
        for buf, dev, early, late, o in (
            (ring_r, right, lo, hi, hops + 1 - h),
            (ring_l, left, hi, lo, (chips - hops - 1 + h) % chips),
        ):
            if h == 2:
                ring_s[s, o, :, early] = (
                    share(o, early) + buf[s, 0, :, early].astype(F32)
                ).astype(BF16)
                ring_s[s, o, :, late] = share(o, late).astype(BF16)
            elif h > 2:
                ring_s[s, o, :, all_c] = (
                    share(o, all_c) + buf[s, h - 2, :, all_c].astype(F32)
                ).astype(BF16)
            c = early if h == 1 else all_c
            send(
                ring_s.at[s, o, :, c],
                buf.at[s, h - 1, :, c],
                ring_send.at[0],
                r_recv.at[k, h - 1],
                dev,
            )

    def ring_end(k):
        with jax.named_scope(f"re{k}"):
            s, at, cols = rings[k]
            c = pl.ds(at, cols)
            hop_wait(k, hops)
            return (
                keep[s, pl.ds(0, TILE), c]
                + pair_r[s, pl.ds(0, TILE), c].astype(F32)
                + ring_r[s, hops - 1, :, c].astype(F32)
                + ring_l[s, hops - 1, :, c].astype(F32)
            )

    set_rings = {}
    for k, (s, _, _) in enumerate(rings):
        set_rings.setdefault(s, []).append(k)
    first_rings = set_rings[0]
    loads["ow"].wait()
    step_w = min(512, width)
    for k in first_rings:
        _, at, cols = rings[k]
        for n in range(cols // step_w):
            c = pl.ds(at + n * step_w, step_w)
            pair_s[0, :, c] = jnp.dot(
                sel[1], ow[:, c], preferred_element_type=F32
            ).astype(BF16)
        pair_start(k)
    @pl.when(sp == last)
    def _():
        pl.semaphore_wait(all_sem, 1)
        for there in range(last):
            pl.semaphore_signal(
                all_sem, inc=1, device_id={"sp": there}, device_id_type=MESH
            )

    for n in range(width // step_w):
        c = pl.ds(n * step_w, step_w)
        keep[0, :, c] = jnp.dot(sel[0], ow[:, c], preferred_element_type=F32)
    for h in range(1, hops + 1):
        for k in first_rings:
            ring_step(k, h)

    loads["routes"].wait()
    loads["route_w"].wait()
    for k in range(TOP):
        for part in range(parts):
            c = pl.ds(part * LANES, LANES)
            table[pl.ds(k * parts + part, 1), :] = routes[pl.ds(k, 1), c].astype(F32)
            table[pl.ds((TOP + k) * parts + part, 1), :] = route_w[pl.ds(k, 1), c]
    columns[:, pl.ds(0, 2 * TOP * parts)] = table[...].T
    base = tp * rows
    my_part = lax.div(base, LANES)
    mine = columns[pl.ds(pl.multiple_of(base - my_part * LANES, rows), rows), :]

    def column(n):
        found = mine[:, n * parts : n * parts + 1]
        for part in range(1, parts):
            found = jnp.where(
                my_part == part, mine[:, n * parts + part : n * parts + part + 1], found
            )
        return found

    lane = lax.broadcasted_iota(jnp.int32, (rows, LANES), 1)
    pos = jnp.floor((lane.astype(F32) + 0.5) * (1.0 / cap)).astype(jnp.int32)
    depth = (lane - pos * cap).astype(F32)
    expert = jnp.where(lane < slots, pos, -1).astype(F32)
    first = (column(0) == expert).astype(F32)
    second = (column(1) == expert).astype(F32)
    named = first + second
    r_at = lax.broadcasted_iota(jnp.int32, (rows, rows), 0)
    c_at = lax.broadcasted_iota(jnp.int32, (rows, rows), 1)
    earlier = (c_at < r_at).astype(F32).astype(BF16)
    rank = jnp.dot(earlier, named.astype(BF16), preferred_element_type=F32)
    hit = named * (rank == depth).astype(F32)
    w_first, w_second = column(TOP), column(TOP + 1)
    w_sum = w_first + w_second
    mix_w = hit * (first * (w_first / w_sum) + second * (w_second / w_sum))
    pick = hit.T.astype(BF16)[:slots, :]

    loads["gains"].wait()
    loads["resid"].wait()
    gain_rows = gains[...]
    projected = jnp.concatenate([ring_end(k) for k in first_rings], axis=1)
    stream = resid[...].astype(F32) + rms_scale(projected, gain_rows[0:1, :])
    stream_ref[...] = stream
    normed = rms_scale(stream, gain_rows[1:2, :]).astype(BF16)

    outgoing = jnp.dot(pick, normed, preferred_element_type=F32)
    for b in range(folds):
        fold[pl.ds(b, slots, stride=folds), :] = outgoing[
            :, b * LANES : (b + 1) * LANES
        ]
    folded = fold[...].astype(BF16)
    zs[...] = folded
    shift = 3 * n_sp // 16
    my_pos = lax.rem(sp + n_sp - shift, n_sp)
    as_source = pl.ds(pl.multiple_of(my_pos * piece, piece), piece)
    as_expert = pl.ds(pl.multiple_of(sp * piece, piece), piece)
    zr[as_source, :] = zs[as_expert, :]

    with jax.named_scope("above"):

        @pl.when(has_above)
        def _():
            pl.semaphore_wait(all_sem, 1)

    for p in reversed(range(1, n_sp)):
        d = (p + 1) // 2 if p % 2 else -(p // 2)
        there = lax.rem(sp + d + n_sp, n_sp)
        send(
            zs.at[pl.ds(pl.multiple_of(there * piece, piece), piece), :],
            zr.at[as_source, :],
            z_send.at[0],
            z_recv.at[my_pos],
            {"sp": there},
        )

    came = set()

    def block(cc, other, o):
        return pl.ds(cc * chunk_rows + other * own_rows + (o % chips) * TILE, TILE)

    part_w = width // 2

    def to_partner(cc, part, o):
        c = pl.ds(part * part_w, part_w)
        send(
            xbuf.at[block(cc, 0, o), c],
            xbuf.at[block(cc, 1, o), c],
            gather_send.at[0],
            d_recv.at[cc],
            partner,
        )

    def gather_hop(cc, part, h):
        with jax.named_scope(f"ag{cc}{part}{h}"):
            gather_step(cc, part, h)

    def arrive(src):
        @pl.when(my_pos != src)
        def _():
            settle(zr.at[pl.ds(src * piece, piece), :], z_recv.at[src])

    def gather_step(cc, part, h):
        if h == 1 and part == 0:
            for src in range(n_sp):
                if src not in came and src * piece < (cc + 1) * span:
                    came.add(src)
                    arrive(src)
            fold[pl.ds(cc * span, span), :] = zr[pl.ds(cc * span, span), :].astype(F32)
            for b in range(folds):
                xbuf[block(cc, 0, 0), pl.ds(b * LANES, LANES)] = fold[
                    pl.ds(cc * span + b, TILE, stride=folds), :
                ].astype(BF16)
        elif h > 1:
            settle(
                xbuf.at[pl.ds(0, 2 * TILE), pl.ds(0, part_w)],
                a_recv.at[cc * 2 + part, h - 2],
            )
        for sign, dev, half in ((-1, right, 0), (1, left, 1)):
            c = pl.ds(part * part_w, part_w)
            if h == hops:
                c = pl.ds(part * part_w + half * (part_w // 2), part_w // 2)
            send(
                xbuf.at[block(cc, 0, sign * (h - 1)), c],
                xbuf.at[block(cc, 0, sign * h), c],
                gather_send.at[0],
                a_recv.at[cc * 2 + part, h - 1],
                dev,
            )
        to_partner(cc, part, 1 - h)
        if h > 1:
            to_partner(cc, part, h - 1)

    def gather_last(cc, part):
        with jax.named_scope(f"al{cc}{part}"):
            settle(
                xbuf.at[pl.ds(0, TILE), pl.ds(0, part_w)],
                a_recv.at[cc * 2 + part, hops - 1],
            )
            to_partner(cc, part, hops)

    def experts(cc):
        s = cc + 1
        with jax.named_scope(f"exw{cc}"):
            settle(
                xbuf.at[pl.ds(cc * chunk_rows + own_rows, own_rows), :], d_recv.at[cc]
            )
        with jax.named_scope(f"exc{cc}"):
            x = xbuf[pl.ds(cc * chunk_rows, chunk_rows), :]
            g = jnp.dot(x, wg[...], preferred_element_type=F32)
            u = jnp.dot(x, wu[...], preferred_element_type=F32)
            hid[...] = (g / (1.0 + jnp.exp(-g)) * u).astype(BF16)
            for k in set_rings[s]:
                _, at, cols = rings[k]
                for n in range(cols // step_w):
                    c = pl.ds(at + n * step_w, step_w)
                    pair_s[s, :, c] = jnp.dot(
                        hid[pl.ds(own_rows, own_rows), :],
                        wd[:, c],
                        preferred_element_type=F32,
                    ).astype(BF16)
                pair_start(k)
            for n in range(width // step_w):
                c = pl.ds(n * step_w, step_w)
                keep[s, :, c] = jnp.dot(
                    hid[pl.ds(0, own_rows), :], wd[:, c], preferred_element_type=F32
                )

    finished = set()
    back_sent = set()
    ended = {}

    def finish(cc, part):
        k = set_rings[cc + 1][part]
        total = ring_end(k)
        first_fold = rings[k][1] // LANES
        for b in range(rings[k][2] // LANES):
            fold[pl.ds(cc * span + first_fold + b, TILE, stride=folds), :] = total[
                :, b * LANES : (b + 1) * LANES
            ]
        ended[cc] = ended.get(cc, 0) + 1
        if ended[cc] < len(set_rings[cc + 1]):
            return
        at = pl.ds(cc * span, span)
        bs[at, :] = fold[at, :].astype(BF16)
        finished.add(cc)
        for p in range(n_sp):
            needs = {p * piece // span, ((p + 1) * piece - 1) // span}
            if p not in back_sent and needs <= finished:
                back_sent.add(p)

                owner = (p + shift) % n_sp

                @pl.when(sp != owner)
                def _():
                    send(
                        bs.at[pl.ds(p * piece, piece), :],
                        br.at[as_expert, :],
                        z_send.at[1],
                        back_recv.at[0],
                        {"sp": owner},
                    )

    for name in ("wg", "wu", "wd"):
        loads[name].wait()
    for op in ORDER:
        if op[0] == 0:
            gather_hop(*op[1:])
        elif op[0] == 4:
            gather_last(*op[1:])
        elif op[0] == 1:
            experts(*op[1:])
        elif op[0] == 2:
            ring_step(set_rings[op[1] + 1][op[2]], op[3])
        else:
            finish(*op[1:])
    br[as_expert, :] = bs[as_source, :]

    far = (n_sp - 1) * piece
    ring_rows = (2 * hops - 1) * TILE
    with jax.named_scope("sendwait"):
        settle(pair_s, pair_send.at[0])
        settle(pair_s.at[:, pl.ds(0, ring_rows), :], ring_send.at[0])
        settle(
            xbuf.at[pl.ds(0, chunks * (ring_rows + own_rows)), :], gather_send.at[0]
        )
        settle(zs.at[pl.ds(piece, far), :], z_send.at[0])

        @pl.when(has_above)
        def _():
            halo.wait_send()

    with jax.named_scope("backwait"):
        settle(br.at[pl.ds(piece, far), :], back_recv.at[0])
    fold[...] = br[...].astype(F32)
    for b in range(folds):
        back[:, pl.ds(b * LANES, LANES)] = fold[
            pl.ds(b, slots, stride=folds), :
        ].astype(BF16)
    mix_w = mix_w[:, :slots]
    mix_hi = mix_w.astype(BF16)
    mix_lo = (mix_w - mix_hi.astype(F32)).astype(BF16)
    picked = back[...]
    combined = jnp.dot(mix_hi, picked, preferred_element_type=F32) + jnp.dot(
        mix_lo, picked, preferred_element_type=F32
    )
    out[...] = stream_ref[...] + rms_scale(combined, gain_rows[2:3, :])
    settle(bs.at[pl.ds(piece, far), :], z_send.at[1])


def per_device(
    resid,
    gate_b,
    gate_c,
    value,
    taps,
    doc_ids,
    out_weight,
    norm_gains,
    routes,
    route_weights,
    w_gate,
    w_up,
    w_down,
):
    n_sp, n_tp = lax.axis_size("sp"), lax.axis_size("tp")
    tok, ch = gate_b.shape
    rows, width = resid.shape
    units = w_gate.shape[2]
    cap = max(2, 3 * TOP * rows // (2 * n_sp))
    chips = n_tp // 2
    hops = chips // 2
    slots = n_sp * cap
    chunks = slots // TILE
    folds = width // LANES
    sets = chunks + 1
    own_rows = chips * TILE
    parts = tok // LANES
    rings = [(0, k * (width // 4), width // 4) for k in range(4)]
    for s in range(1, sets):
        rings += [(s, k * (width // 2), width // 2) for k in range(2)]
    n_rings = len(rings)
    operands = (
        resid,
        gate_b,
        gate_c,
        value,
        taps,
        doc_ids.reshape(parts, LANES),
        out_weight,
        norm_gains,
        routes.T,
        route_weights.T,
        w_gate,
        w_up,
        w_down,
    )
    hbm = pl.BlockSpec(memory_space=pl.ANY)
    vmem = pltpu.VMEM
    dma = pltpu.SemaphoreType.DMA
    result = pl.pallas_call(
        functools.partial(layer_kernel, n_sp, n_tp, cap, rings),
        out_shape=jax.ShapeDtypeStruct((rows, width), F32),
        in_specs=[hbm] * len(operands),
        out_specs=pl.BlockSpec(memory_space=vmem),
        scratch_shapes=[
            *[vmem(a.shape, a.dtype) for a in operands[:10]],
            *[vmem(a.shape[1:], a.dtype) for a in operands[10:]],
            vmem((tok + 8, ch), F32),
            vmem((tok + 8, LANES), F32),
            vmem((16, ch), F32),
            vmem((16, ch), F32),
            vmem((tok, ch), BF16),
            vmem((2, own_rows, ch), BF16),
            vmem((2 * TOP * parts, LANES), F32),
            vmem((LANES, LANES), F32),
            vmem((slots * folds, LANES), BF16),
            vmem((slots * folds, LANES), BF16),
            vmem((slots * folds, LANES), BF16),
            vmem((slots * folds, LANES), BF16),
            vmem((slots * folds, LANES), F32),
            vmem((chunks * n_tp * TILE, width), BF16),
            vmem((n_tp * TILE, units), BF16),
            vmem((sets, own_rows, width), BF16),
            vmem((sets, own_rows, width), BF16),
            vmem((sets, own_rows, width), F32),
            vmem((sets, chips, TILE, width), BF16),
            vmem((sets, hops, TILE, width), BF16),
            vmem((sets, hops, TILE, width), BF16),
            vmem((rows, width), F32),
            vmem((slots, width), BF16),
            dma((len(operands),)),
            dma((2,)),
            pltpu.SemaphoreType.REGULAR,
            pltpu.SemaphoreType.REGULAR,
            dma((2,)),
            dma((n_sp,)),
            dma((1,)),
            dma((1,)),
            dma((n_rings,)),
            dma((1,)),
            dma((n_rings, hops)),
            dma((1,)),
            dma((chunks,)),
            dma((chunks * 2, hops)),
        ],
        compiler_params=pltpu.CompilerParams(
            collective_id=0,
            has_side_effects=True,
            vmem_limit_bytes=56 * 1024 * 1024,
        ),
        name="layer",
    )(*operands)
    return result.astype(BF16)


def solution(mesh):
    return jax.shard_map(
        per_device,
        mesh=mesh,
        in_specs=(
            P(("grp", "sp", "tp"), None),
            P(("grp", "sp"), "tp"),
            P(("grp", "sp"), "tp"),
            P(("grp", "sp"), "tp"),
            P(None, "tp"),
            P(("grp", "sp")),
            P("tp", None),
            P(),
            P(("grp", "sp"), None),
            P(("grp", "sp"), None),
            P("sp", None, "tp"),
            P("sp", None, "tp"),
            P("sp", "tp", None),
        ),
        out_specs=P(("grp", "sp", "tp"), None),
        check_vma=False,
    )
```
